32 devices in a mesh: ep: 8 (over z, y), tp: 4 (over x, core).
Axes of the slice: x: 2, y: 2, z: 4, core: 2. Of those that a mesh axis runs over, the one named last changes fastest.
Arguments:
- tokens: bfloat16 [64, 2048], P('ep'), may hold values from -4 to 4
- w_query: bfloat16 [2048, 1024], P(None, 'tp'), may hold values from -0.125 to 0.125
- w_key: bfloat16 [2048, 1024], P(None, 'tp'), may hold values from -0.125 to 0.125
- w_value: bfloat16 [2048, 1024], P(None, 'tp'), may hold values from -0.125 to 0.125
- w_outgate: bfloat16 [2048, 1024], P(None, 'tp'), may hold values from -0.125 to 0.125
- w_igate: bfloat16 [2048, 4], P(None, 'tp'), may hold values from -0.125 to 0.125
- w_fgate: bfloat16 [2048, 4], P(None, 'tp'), may hold values from -0.125 to 0.125
- forget_bias: float32 [4], P('tp'), may hold values from -1 to 5
- w_out: bfloat16 [1024, 2048], P('tp'), may hold values from -0.1875 to 0.1875
- gain_mix: float32 [2048], replicated, may hold values from 0.1 to 1.9
- gain_moe: float32 [2048], replicated, may hold values from 0.1 to 1.9
- memory: float32 [64, 4, 256, 256], P('ep', 'tp'), may hold values from -0.4 to 0.4
- normalizer: float32 [64, 4, 256], P('ep', 'tp'), may hold values from -0.8 to 0.8
- stabilizer: float32 [64, 4], P('ep', 'tp'), may hold values from 0 to 2
- expert_gate: bfloat16 [8, 2048, 512], P('ep', None, 'tp'), may hold values from -0.125 to 0.125
- expert_up: bfloat16 [8, 2048, 512], P('ep', None, 'tp'), may hold values from -0.125 to 0.125
- expert_down: bfloat16 [8, 512, 2048], P('ep', 'tp'), may hold values from -1 to 1
- routes: int32 [64, 4], P('ep'), may hold values from 0 to 7, all different within a row; in each aligned block of 8 rows (0 to 7, 8 to 15, ...) at most 8 rows name the same one
- route_weight: float32 [64, 4], P('ep'), may hold values from 0.2 to 1
Outputs:
- output: bfloat16 [64, 2048], P('ep', 'tp')
- memory_next: float32 [64, 4, 256, 256], P('ep', 'tp')
- norm_next: float32 [64, 4, 256], P('ep', 'tp')
- stabilizer_next: float32 [64, 4], P('ep', 'tp')
The draws below stay inside these ranges and needn't reach their ends.
Inputs may be any that keep to these rules, and one draw needn't show every extreme that they name: `routes`: each row names 4 different experts. Among the 8 rows of one device (aligned blocks), no expert is named more than 8 times, a bound that some block reaches.
All inputs are finite; a program needn't handle non-finite values.
Results may differ from the reference program's by a relative error of at most 0.029.
Values may be sent and summed in bfloat16 or wider, within the bound.
No kernel may reach another device: no remote copies, remote signals or barrier semaphores. Data moves between devices by JAX's collectives and lax.ppermute only.
A program may use at most 64 MiB of HBM per device.

```python
import math
import jax
import jax.numpy as jnp
import numpy as np
from jax import lax

D = 2048
NH = 4
DH = 256
FF = 512
TOP = 4
SEQ_DEV = 8
TOKENS = 64
EXPERTS = 8
CAP = 8
N_EP = 8


def steps_of(stream_key, shape, pieces, least, high):
    loudness = 1.0
    for position, parts in pieces:
        steps = jax.random.uniform(jax.random.fold_in(jax.random.fold_in(stream_key, 6), position), (parts,), jnp.float32, least / len(pieces), high / len(pieces))
        loudness = loudness * jnp.repeat(jnp.exp(steps), shape[position] // parts).reshape((-1,) + (1,) * (len(shape) - 1 - position))
    return loudness


def routed_block(rng, own, number, rows, count, top, reach, slope):
    order = jax.random.permutation(rng, count)
    crowded, ordinary = load_shares(count, rows * top, reach, slope, True), load_shares(count, rows * top, reach, slope, False)
    places = jnp.arange(count)

    def named(tallies, offset_by):
        used = int((tallies > 0).sum())
        fixed = max(1, used // 4)
        passed = fixed + (places - fixed + offset_by * (used - fixed)) % max(1, count - fixed)
        return jnp.zeros((count,), jnp.int32).at[order[jnp.where(places < fixed, places, passed)]].set(jnp.asarray(tallies, jnp.int32))

    tallies = jnp.where(number % 4 == 0, named(crowded, number // 4), named(ordinary, number - number // 4 - 1))
    mixed = jax.random.permutation(jax.random.fold_in(own, 3), count)
    giver, sink = mixed[0:count // 2 * 2:2], mixed[1:count // 2 * 2:2]
    margin = jnp.minimum(tallies[giver] - 1, reach - tallies[sink]) // 2
    margin = jnp.where((giver == order[0]) | (sink == order[0]) | (tallies[sink] == 0), 0, jnp.maximum(margin, 0))
    passed = jax.random.randint(jax.random.fold_in(own, 4), (count // 2,), 0, 1 << 20) % (margin + 1)
    tallies = tallies.at[giver].add(-passed).at[sink].add(passed)
    items = jnp.searchsorted(jnp.cumsum(tallies), jnp.arange(rows * top), side="right").astype(jnp.int32)
    grid = items.reshape(top, rows).T
    grid = grid[jax.random.permutation(jax.random.fold_in(own, 1), rows)]
    offset_by = jax.random.randint(jax.random.fold_in(own, 2), (rows, 1), 0, top)
    return jnp.take_along_axis(grid, (jnp.arange(top)[None, :] + offset_by) % top, axis=1)


def load_shares(count, total, reach, slope, full):
    loads = [(1 << 20) // math.isqrt(standing ** slope) + 1 for standing in range(1, count + 1)]
    largest = reach if full else min(reach, max(-(-total // count), total * loads[0] // sum(loads)))
    least = 1 if total - largest >= count - 1 else 0
    counts, spare = [largest] + [least] * (count - 1), total - largest - least * (count - 1)
    while spare > 0:
        free = [i for i in range(1, count) if counts[i] < largest] or [i for i in range(1, count) if counts[i] < reach]
        mass, left = sum([loads[i] for i in free]), spare
        for i in free:
            more = min(reach - counts[i], max(1, left * loads[i] // mass), spare)
            counts[i] = counts[i] + more
            spare = spare - more
    return np.array(counts)


def scatter_about(stream_key, extent, deviation, reach, split=(), held_as=jnp.bfloat16):
    values = jax.random.normal(stream_key, extent, jnp.float32) * deviation
    if len(split) > 0:
        values = steps_of(stream_key, extent, split, -0.22, 0.18) * values
    return jnp.clip(values, min=-reach, max=reach).astype(held_as)


def setup_inputs(seed: int = 0) -> dict:
    key_list = jax.random.split(jax.random.key(seed), 20)
    tokens = scatter_about(key_list[0], (TOKENS, D), 1.0, 4.0, ((0, 8),))
    w_query = scatter_about(key_list[1], (D, NH * DH), D ** -0.5, 0.125, ((1, 4),))
    w_key = scatter_about(key_list[2], (D, NH * DH), D ** -0.5, 0.125, ((1, 4),))
    w_value = scatter_about(key_list[3], (D, NH * DH), D ** -0.5, 0.125, ((1, 4),))
    w_outgate = scatter_about(key_list[4], (D, NH * DH), D ** -0.5, 0.125, ((1, 4),))
    w_igate = scatter_about(key_list[5], (D, NH), D ** -0.5, 0.125, ((1, 4),))
    w_fgate = scatter_about(key_list[6], (D, NH), D ** -0.5, 0.125, ((1, 4),))
    forget_bias = jnp.clip(-1.0 + 6.0 * jax.random.uniform(key_list[7], (NH,), jnp.float32) ** steps_of(key_list[7], (NH,), ((0, 4),), -0.2, 0.2), -1.0, 5.0)
    w_out = scatter_about(key_list[8], (NH * DH, D), (NH * DH) ** -0.5, 0.1875, ((0, 4),))
    gain_mix = jnp.clip(1.0 + 0.18 * jax.random.normal(key_list[9], (D,), jnp.float32), 0.1, 1.9)
    gain_moe = jnp.clip(1.0 + 0.18 * jax.random.normal(key_list[10], (D,), jnp.float32), 0.1, 1.9)
    memory = scatter_about(key_list[11], (TOKENS, NH, DH, DH), 0.05, 0.4, ((0, 8), (1, 4)), jnp.float32)
    normalizer = scatter_about(key_list[12], (TOKENS, NH, DH), 0.1, 0.8, ((0, 8), (1, 4)), jnp.float32)
    stabilizer = jnp.clip(2.0 * jax.random.uniform(key_list[13], (TOKENS, NH), jnp.float32) ** steps_of(key_list[13], (TOKENS, NH), ((0, 8), (1, 4)), -0.2, 0.2), 0.0, 2.0)
    expert_gate = scatter_about(key_list[14], (EXPERTS, D, FF), D ** -0.5, 0.125, ((0, 8), (2, 4)))
    expert_up = scatter_about(key_list[15], (EXPERTS, D, FF), D ** -0.5, 0.125, ((0, 8), (2, 4)))
    expert_down = scatter_about(key_list[16], (EXPERTS, FF, D), (FF // 16) ** -0.5, 1.0, ((0, 8), (1, 4)))
    routes_keys = jax.random.split(jax.random.fold_in(key_list[17], 1), TOKENS // SEQ_DEV)
    routes_turns = jax.random.permutation(jax.random.fold_in(key_list[17], 3), TOKENS // SEQ_DEV)
    routes = jax.vmap(lambda own, number: routed_block(jax.random.fold_in(key_list[17], 2), own, number, SEQ_DEV, EXPERTS, TOP, CAP, 2))(routes_keys, routes_turns).reshape((TOKENS, TOP))
    route_weight = jnp.clip(0.2 + 0.8 * jax.random.uniform(key_list[18], (TOKENS, TOP), jnp.float32) ** steps_of(key_list[18], (TOKENS, TOP), ((0, 8),), -0.2, 0.2), 0.2, 1.0)
    return dict(tokens=tokens, w_query=w_query, w_key=w_key, w_value=w_value, w_outgate=w_outgate, w_igate=w_igate, w_fgate=w_fgate, forget_bias=forget_bias, w_out=w_out, gain_mix=gain_mix, gain_moe=gain_moe, memory=memory, normalizer=normalizer, stabilizer=stabilizer, expert_gate=expert_gate, expert_up=expert_up, expert_down=expert_down, routes=routes, route_weight=route_weight)


def layer_norm(row_data, gain_vec):
    values = row_data.astype(jnp.float32)
    row_mean = lax.optimization_barrier(jnp.mean(values, -1, keepdims=True))
    centered = values - row_mean
    variance = lax.optimization_barrier(jnp.mean(centered * centered, -1, keepdims=True))
    return centered * lax.rsqrt(variance + 1e-05) * gain_vec

def slot_targets(routes, experts, capacity):
    flat_routes = routes.reshape(-1)
    onehot = (flat_routes[:, None] == jnp.arange(experts, dtype=jnp.int32)[None, :]).astype(jnp.int32)
    before = jnp.cumsum(onehot, axis=0) - onehot
    slot_index = lax.optimization_barrier(jnp.sum(before * onehot, axis=1))
    return (flat_routes * capacity + slot_index).astype(jnp.int32)

def expert_rows(operands):
    rows_in, gate_weight, up_weight, down_weight = operands
    gate_part = jnp.dot(rows_in, gate_weight, preferred_element_type=jnp.float32)
    up_part = jnp.dot(rows_in, up_weight, preferred_element_type=jnp.float32)
    hidden = (jax.nn.silu(gate_part) * up_part).astype(jnp.bfloat16)
    return jnp.dot(hidden, down_weight, preferred_element_type=jnp.float32).astype(jnp.bfloat16)

def reference(tokens, w_query, w_key, w_value, w_outgate, w_igate, w_fgate, forget_bias, w_out, gain_mix, gain_moe, memory, normalizer, stabilizer, expert_gate, expert_up, expert_down, routes, route_weight):
    normed = layer_norm(tokens, gain_mix).astype(jnp.bfloat16)

    def project(weight):
        rounded = jnp.dot(normed, weight, preferred_element_type=jnp.float32).astype(jnp.bfloat16)
        rounded = lax.optimization_barrier(rounded)
        return rounded.astype(jnp.float32).reshape(TOKENS, NH, DH)
    queries = project(w_query)
    keys_scaled = project(w_key) / math.sqrt(DH)
    values_rows = project(w_value)
    out_gate = project(w_outgate)
    gate_in = jnp.dot(normed, w_igate, preferred_element_type=jnp.float32)
    gate_forget = jnp.dot(normed, w_fgate, preferred_element_type=jnp.float32)
    log_forget = jax.nn.log_sigmoid(gate_forget + forget_bias)
    stabilizer_next = jnp.maximum(log_forget + stabilizer, gate_in)
    keep_rate = jnp.exp(log_forget + stabilizer - stabilizer_next)
    admit_rate = jnp.exp(gate_in - stabilizer_next)
    memory_next = keep_rate[:, :, None, None] * memory + admit_rate[:, :, None, None] * keys_scaled[:, :, :, None] * values_rows[:, :, None, :]
    norm_next = keep_rate[:, :, None] * normalizer + admit_rate[:, :, None] * keys_scaled
    numerator = jnp.einsum('thk,thkv->thv', queries, memory_next, precision=lax.Precision.HIGHEST)
    denominator = lax.optimization_barrier(jnp.sum(queries * norm_next, axis=-1))
    readout = numerator / jnp.maximum(jnp.abs(denominator), jnp.exp(-stabilizer_next))[:, :, None]
    mixed = (jax.nn.sigmoid(out_gate) * readout).astype(jnp.bfloat16)
    head_part = jnp.einsum('thd,hde->the', mixed.astype(jnp.float32), w_out.reshape(NH, DH, D).astype(jnp.float32)).astype(jnp.bfloat16)
    residual = tokens.astype(jnp.float32) + lax.optimization_barrier(jnp.sum(head_part.astype(jnp.float32), axis=1))
    expert_in = layer_norm(residual, gain_moe).astype(jnp.bfloat16)
    blocks = routes.reshape(N_EP, SEQ_DEV * TOP)
    local_target = jax.vmap(lambda route_row: slot_targets(route_row, EXPERTS, CAP))(blocks)
    slot_index = local_target - blocks * CAP
    block_index = jnp.arange(N_EP, dtype=jnp.int32)[:, None]
    placement = ((blocks * N_EP + block_index) * CAP + slot_index).reshape(-1).astype(jnp.int32)
    buffer = jnp.zeros((EXPERTS * N_EP * CAP, D), jnp.bfloat16).at[placement].set(jnp.repeat(expert_in, TOP, axis=0))
    expert_outs = lax.map(expert_rows, (buffer.reshape(EXPERTS, N_EP * CAP, D), expert_gate, expert_up, expert_down))
    picked = expert_outs.reshape(-1, D)[placement].reshape(TOKENS, TOP, D)
    combined = lax.optimization_barrier(jnp.sum(route_weight[:, :, None] * picked.astype(jnp.float32), axis=1))
    output = (residual + combined).astype(jnp.bfloat16)
    return (output, memory_next, norm_next, stabilizer_next)
```

```python
import math

import jax
import jax.numpy as jnp
from jax import lax
from jax.sharding import PartitionSpec as P

BOTH = ("ep", "tp")


def layer_norm(row_data, gain_vec):
    values = row_data.astype(jnp.float32)
    row_mean = jnp.mean(values, -1, keepdims=True)
    centered = values - row_mean
    variance = jnp.mean(centered * centered, -1, keepdims=True)
    return centered * lax.rsqrt(variance + 1e-05) * gain_vec


def shards(
    tokens,
    w_query,
    w_key,
    w_value,
    w_outgate,
    w_igate,
    w_fgate,
    forget_bias,
    w_out,
    gain_mix,
    gain_moe,
    memory,
    normalizer,
    stabilizer,
    expert_gate,
    expert_up,
    expert_down,
    routes,
    route_weight,
):
    ep_size = lax.axis_size("ep")
    tp_size = lax.axis_size("tp")
    seq_rows, model_width = tokens.shape
    head_count = memory.shape[1]
    head_size = memory.shape[2]
    head_cols = head_count * head_size
    quarter = model_width // tp_size
    half = seq_rows // 2
    duo = tp_size // 2
    ep_id = lax.axis_index("ep")
    tp_id = lax.axis_index("tp")
    side = tp_id % 2
    swap = [(t, t ^ 1) for t in range(tp_size)]
    same_side = [
        [e * tp_size + x * 2 + c for e in range(ep_size) for x in range(duo)] for c in range(2)
    ]
    mate_gate = lax.ppermute(expert_gate[0], "tp", swap)
    mate_up = lax.ppermute(expert_up[0], "tp", swap)
    mate_down = lax.ppermute(expert_down[0], "tp", swap)

    normed = layer_norm(tokens, gain_mix).astype(jnp.bfloat16)
    gate_in = jnp.dot(normed, w_igate, preferred_element_type=jnp.float32)
    gate_forget = jnp.dot(normed, w_fgate, preferred_element_type=jnp.float32)
    queries, keys, values_rows, out_gate = [
        jnp.dot(normed, weight, preferred_element_type=jnp.float32)
        .astype(jnp.bfloat16)
        .astype(jnp.float32)
        .reshape(seq_rows, head_count, head_size)
        for weight in (w_query, w_key, w_value, w_outgate)
    ]
    keys_scaled = keys / math.sqrt(head_size)
    log_forget = jax.nn.log_sigmoid(gate_forget + forget_bias)
    stabilizer_next = jnp.maximum(log_forget + stabilizer, gate_in)
    keep_rate = jnp.exp(log_forget + stabilizer - stabilizer_next)
    admit_rate = jnp.exp(gate_in - stabilizer_next)
    memory_next = (
        keep_rate[:, :, None, None] * memory
        + admit_rate[:, :, None, None] * keys_scaled[:, :, :, None] * values_rows[:, :, None, :]
    )
    norm_next = keep_rate[:, :, None] * normalizer + admit_rate[:, :, None] * keys_scaled
    numerator = jnp.einsum("shk,shkv->shv", queries, memory_next, precision=lax.Precision.HIGHEST)
    denominator = jnp.sum(queries * norm_next, axis=-1)
    readout = numerator / jnp.maximum(jnp.abs(denominator), jnp.exp(-stabilizer_next))[:, :, None]
    mixed = (jax.nn.sigmoid(out_gate) * readout).astype(jnp.bfloat16).reshape(seq_rows, head_cols)
    head_part = jnp.dot(mixed, w_out, preferred_element_type=jnp.float32)
    own_token = jnp.where(tp_id < 2, 1.0, 0.0) * tokens.astype(jnp.float32)

    first = side == 0
    sent = jnp.where(first, head_part[half:], head_part[:half]).astype(jnp.bfloat16)
    kept = head_part + own_token
    kept = jnp.where(first, kept[:half], kept[half:])
    met = lax.ppermute(sent, "tp", swap)
    pair_sum = (kept + met.astype(jnp.float32)).astype(jnp.bfloat16)
    outbound = jnp.broadcast_to(pair_sum[None], (ep_size * duo, half, model_width))
    arrived = lax.all_to_all(
        outbound, BOTH, 0, 0, tiled=True, axis_index_groups=same_side
    )
    residual = jnp.sum(
        arrived.reshape(ep_size, duo, half, model_width).astype(jnp.float32), axis=1
    )
    own_rows = lax.dynamic_index_in_dim(residual, ep_id, 0, keepdims=False)
    for_mate = lax.dynamic_slice_in_dim(own_rows, (tp_id ^ 1) * quarter, quarter, 1)
    for_self = lax.dynamic_slice_in_dim(own_rows, tp_id * quarter, quarter, 1)
    from_mate = lax.ppermute(for_mate, "tp", swap)

    expert_in = layer_norm(residual.reshape(-1, model_width), gain_moe).astype(jnp.bfloat16)

    def one(gate_w, up_w, down_w):
        gate_part = jnp.dot(expert_in, gate_w, preferred_element_type=jnp.float32)
        up_part = jnp.dot(expert_in, up_w, preferred_element_type=jnp.float32)
        hidden = (jax.nn.silu(gate_part) * up_part).astype(jnp.bfloat16)
        return jnp.dot(hidden, down_w, preferred_element_type=jnp.float32)

    part = one(expert_gate[0], expert_up[0], expert_down[0]) + one(mate_gate, mate_up, mate_down)
    blocks = (
        part.astype(jnp.bfloat16)
        .reshape(ep_size, half, tp_size, quarter)
        .transpose(0, 2, 1, 3)
        .reshape(ep_size * tp_size, half, quarter)
    )
    returned = lax.all_to_all(blocks, BOTH, 0, 0, tiled=True)
    per_expert = jnp.sum(
        returned.reshape(ep_size, duo, 2, half, quarter).astype(jnp.float32), axis=1
    )
    share = jnp.sum(
        jnp.where(
            routes[:, :, None] == jnp.arange(ep_size, dtype=jnp.int32)[None, None, :],
            route_weight[:, :, None],
            0.0,
        ),
        axis=1,
    )
    combined = jnp.sum(
        share.T[:, :, None] * per_expert.reshape(ep_size, seq_rows, quarter), axis=0
    )
    own_cols = jnp.concatenate(
        [jnp.where(first, for_self, from_mate), jnp.where(first, from_mate, for_self)], axis=0
    )
    output = (own_cols + combined).astype(jnp.bfloat16)
    return (output, memory_next, norm_next, stabilizer_next)


def solution(mesh):
    return jax.shard_map(
        shards,
        mesh=mesh,
        in_specs=(
            P("ep", None),
            P(None, "tp"),
            P(None, "tp"),
            P(None, "tp"),
            P(None, "tp"),
            P(None, "tp"),
            P(None, "tp"),
            P("tp"),
            P("tp", None),
            P(),
            P(),
            P("ep", "tp", None, None),
            P("ep", "tp", None),
            P("ep", "tp"),
            P("ep", None, "tp"),
            P("ep", None, "tp"),
            P("ep", "tp", None),
            P("ep", None),
            P("ep", None),
        ),
        out_specs=(P("ep", "tp"), P("ep", "tp", None, None), P("ep", "tp", None), P("ep", "tp")),
        check_vma=False,
    )
```

```python
import functools
import math

import jax
import jax.numpy as jnp
from jax import lax
from jax.experimental import pallas as pl
from jax.experimental.pallas import tpu as pltpu
from jax.sharding import PartitionSpec as P


BOTH = ("ep", "tp")
F32 = jnp.float32
BF16 = jnp.bfloat16


def dot(left, right):
    return jnp.dot(left, right, preferred_element_type=F32)


def normalize(values, gain_row):
    centered = values - jnp.mean(values, -1, keepdims=True)
    variance = jnp.mean(centered * centered, -1, keepdims=True)
    return centered * lax.rsqrt(variance + 1e-05) * gain_row


def eye_mask(size):
    rows = lax.broadcasted_iota(jnp.int32, (size, size), 0)
    return rows == lax.broadcasted_iota(jnp.int32, (size, size), 1)


def as_column(row):
    size = row.shape[1]
    spread = jnp.broadcast_to(row, (size, size))
    return jnp.sum(jnp.where(eye_mask(size), spread, 0.0), axis=1, keepdims=True)


def as_row(column):
    size = column.shape[0]
    spread = jnp.broadcast_to(column, (size, size))
    return jnp.sum(jnp.where(eye_mask(size), spread, 0.0), axis=0, keepdims=True)


def cell_kernel(
    bias,
    tokens_hbm,
    gain_hbm,
    w_in_hbm,
    w_forget_hbm,
    stabilizer_hbm,
    normalizer_hbm,
    wq_hbm,
    wk_hbm,
    wv_hbm,
    memory_hbm,
    wo_hbm,
    w_out_hbm,
    routes_hbm,
    route_weight_hbm,
    sent,
    kept,
    tags,
    norm_next,
    stabilizer_next,
    keep_out,
    fresh_out,
    values_out,
    tokens,
    gain,
    w_in,
    w_forget,
    stabilizer,
    normalizer,
    wq,
    wk,
    wv,
    memory,
    wo,
    w_out,
    routes,
    route_weight,
    sems,
    *,
    experts,
):
    pairs = (
        (tokens_hbm, tokens),
        (gain_hbm, gain),
        (w_in_hbm, w_in),
        (w_forget_hbm, w_forget),
        (stabilizer_hbm, stabilizer),
        (normalizer_hbm, normalizer),
        (wq_hbm, wq),
        (wk_hbm, wk),
        (wv_hbm, wv),
        (wo_hbm, wo),
        (w_out_hbm, w_out),
        (routes_hbm, routes),
        (route_weight_hbm, route_weight),
        (memory_hbm, memory),
    )
    copies = [
        pltpu.make_async_copy(src, dst, sems.at[n]) for n, (src, dst) in enumerate(pairs)
    ]
    tp_id = lax.axis_index("tp")
    early = (0, 1, 2, 3, 4, 5, 11, 12)
    for n in early + (6, 7, 8, 13, 9, 10):
        copies[n].start()
    for n in early:
        copies[n].wait()
    seq_rows = tokens.shape[0]
    half = seq_rows // 2
    head_size = memory.shape[-1]
    token_rows = tokens[...].astype(F32)
    normed = normalize(token_rows, gain[...]).astype(BF16)
    wide = normed.astype(F32)
    gate_in = jnp.sum(wide * w_in[...].astype(F32), axis=1, keepdims=True)
    gate_forget = jnp.sum(wide * w_forget[...].astype(F32), axis=1, keepdims=True)
    logit = gate_forget + bias[0]
    log_forget = jnp.minimum(logit, 0.0) - jnp.log1p(jnp.exp(-jnp.abs(logit)))
    shifted = log_forget + as_column(stabilizer[...])
    stab = jnp.maximum(shifted, gate_in)
    keep = jnp.exp(shifted - stab)
    admit = jnp.exp(gate_in - stab)
    stabilizer_next[...] = as_row(stab)
    keep_out[...] = as_row(keep)

    def project(number, weight):
        copies[number].wait()
        return dot(normed, weight[...]).astype(BF16).astype(F32)

    queries = project(6, wq)
    columns = queries.T
    keys = project(7, wk) * (1.0 / math.sqrt(head_size))
    values = project(8, wv)
    fresh = admit * keys
    grown = keep * normalizer[...].reshape(seq_rows, head_size) + fresh
    norm_next[...] = grown.reshape(norm_next.shape)
    fresh_out[...] = fresh
    values_out[...] = values
    match = jnp.sum(queries * fresh, axis=1, keepdims=True)
    divisor = jnp.maximum(
        jnp.abs(jnp.sum(queries * grown, axis=1, keepdims=True)), jnp.exp(-stab)
    )
    named = routes[...].astype(F32)
    lanes = lax.broadcasted_iota(jnp.int32, (seq_rows, tags.shape[1]), 1)
    expert_of = (lanes % experts).astype(F32)
    share = jnp.zeros(lanes.shape, F32)
    for k in range(routes.shape[0]):
        share = share + jnp.where(
            expert_of == as_column(named[k : k + 1]), as_column(route_weight[k : k + 1]), 0.0
        )
    coarse = share.astype(BF16).astype(F32)
    share = jnp.where(lanes < experts, coarse, share - coarse)
    share = jnp.where(lanes < 2 * experts, share, 0.0).astype(BF16)
    copies[13].wait()
    recalled = []
    for s in range(seq_rows):
        recalled.append(jnp.sum(columns[:, s : s + 1] * memory[s, 0], axis=0, keepdims=True))
    old = jnp.concatenate(recalled, axis=0)
    readout = (keep * old + match * values) / divisor
    out_gate = project(9, wo)
    mixed = (jax.nn.sigmoid(out_gate) * readout).astype(BF16)
    copies[10].wait()
    head_part = dot(mixed, w_out[...])
    first = tp_id & 1 == 0
    own = head_part + jnp.where(tp_id < 2, 1.0, 0.0) * token_rows

    @pl.when(first)
    def _():
        sent[...] = head_part[half:].astype(BF16)
        kept[...] = own[:half]
        tags[...] = share[:half]

    @pl.when(jnp.logical_not(first))
    def _():
        sent[...] = head_part[:half].astype(BF16)
        kept[...] = own[half:]
        tags[...] = share[half:]


def spread_kernel(kept, met, tags, outbound):
    width = kept.shape[1]
    pair_sum = (kept[...] + met[...].astype(F32)).astype(BF16)
    for n in range(outbound.shape[0]):
        outbound[n, :, :width] = pair_sum
        outbound[n, :, width:] = tags[...]


def load_kernel(*refs):
    count = len(refs) // 2
    sems = refs[-1]
    copies = [
        pltpu.make_async_copy(refs[n], refs[count + n], sems.at[n]) for n in range(count)
    ]
    for copy in copies:
        copy.start()
    for copy in copies:
        copy.wait()


def expert_kernel(
    arrived,
    gain,
    gate_a,
    up_a,
    down_a,
    gate_b,
    up_b,
    down_b,
    blocks,
    residual,
    tags,
):
    half, quarter = blocks.shape[1:]
    width = residual.shape[1]
    rows = residual.shape[0]
    ep_size = rows // half
    duo = arrived.shape[0] // ep_size
    tp_size = width // quarter
    for e in range(ep_size):
        total = arrived[e * duo, :, :width].astype(F32)
        for x in range(1, duo):
            total = total + arrived[e * duo + x, :, :width].astype(F32)
        residual[e * half : (e + 1) * half, :] = total
        tags[e * half : (e + 1) * half, :] = arrived[e * duo, :, width:].astype(F32)
    ep_id = lax.axis_index("ep")
    lanes = lax.broadcasted_iota(jnp.int32, tags.shape, 1)
    chosen = (lanes == ep_id) | (lanes == ep_id + ep_size)
    share = jnp.sum(jnp.where(chosen, tags[...], 0.0), axis=1, keepdims=True)
    owner = lax.broadcasted_iota(jnp.int32, (rows, 1), 0) // half
    carried = jnp.where((owner == ep_id) & (lax.axis_index("tp") < 2), 1.0, 0.0)
    rows_in = normalize(residual[...], gain[...]).astype(BF16)

    def hidden(gate, up):
        both = dot(rows_in, jnp.concatenate([gate[...], up[...]], axis=1))
        gate_part, up_part = jnp.split(both, 2, axis=1)
        return (gate_part * jax.nn.sigmoid(gate_part) * up_part).astype(BF16)

    hiddens = jnp.concatenate([hidden(gate_a, up_a), hidden(gate_b, up_b)], axis=1)
    part = dot(hiddens, jnp.concatenate([down_a[...], down_b[...]], axis=0))
    part = share * part + carried * residual[...]
    for e in range(ep_size):
        for t in range(tp_size):
            piece = part[e * half : (e + 1) * half, t * quarter : (t + 1) * quarter]
            blocks[e * tp_size + t] = piece.astype(BF16)


def combine_kernel(returned, output):
    half = returned.shape[1]
    for c in range(2):
        total = returned[c].astype(F32)
        for n in range(c + 2, returned.shape[0], 2):
            total = total + returned[n].astype(F32)
        output[c * half : (c + 1) * half, :] = total.astype(BF16)


def shards(
    tokens,
    w_query,
    w_key,
    w_value,
    w_outgate,
    w_igate,
    w_fgate,
    forget_bias,
    w_out,
    gain_mix,
    gain_moe,
    memory,
    normalizer,
    stabilizer,
    expert_gate,
    expert_up,
    expert_down,
    routes,
    route_weight,
):
    ep_size = lax.axis_size("ep")
    tp_size = lax.axis_size("tp")
    seq_rows, width = tokens.shape
    head_size = memory.shape[2]
    quarter = width // tp_size
    half = seq_rows // 2
    duo = tp_size // 2
    swap = [(t, t ^ 1) for t in range(tp_size)]
    same_side = [
        [e * tp_size + x * 2 + c for e in range(ep_size) for x in range(duo)] for c in range(2)
    ]
    smem = pl.BlockSpec(memory_space=pltpu.SMEM)
    vmem = pl.BlockSpec(memory_space=pltpu.VMEM)
    hbm = pl.BlockSpec(memory_space=pltpu.HBM)

    def room(kib):
        return pltpu.CompilerParams(vmem_limit_bytes=kib * 1024)

    shape = jax.ShapeDtypeStruct
    loads = (
        tokens,
        gain_mix.reshape(1, -1),
        w_igate.T,
        w_fgate.T,
        stabilizer.T,
        normalizer,
        w_query,
        w_key,
        w_value,
        memory,
        w_outgate,
        w_out,
        routes.T,
        route_weight.T,
    )
    tag_width = -(-2 * ep_size // 128) * 128
    sent, kept, tags, norm_next, stab_row, keep, fresh, values = pl.pallas_call(
        functools.partial(cell_kernel, experts=ep_size),
        out_shape=(
            shape((half, width), BF16),
            shape((half, width), F32),
            shape((half, tag_width), BF16),
            shape(normalizer.shape, F32),
            shape((1, seq_rows), F32),
            shape((1, seq_rows), F32),
            shape((seq_rows, head_size), F32),
            shape((seq_rows, head_size), F32),
        ),
        in_specs=[smem] + [hbm] * len(loads),
        out_specs=(vmem,) * 8,
        scratch_shapes=[pltpu.VMEM(array.shape, array.dtype) for array in loads]
        + [pltpu.SemaphoreType.DMA((len(loads),))],
        compiler_params=room(20480),
        name="cell",
    )(
        forget_bias,
        *[pltpu.with_memory_space_constraint(array, pltpu.HBM) for array in loads],
    )
    weights = (expert_gate[0], expert_up[0], expert_down[0])
    sent, weights = lax.optimization_barrier((sent, weights))
    met = lax.ppermute(sent, "tp", swap)
    mates = [lax.ppermute(weight, "tp", swap) for weight in weights]
    outbound = pl.pallas_call(
        spread_kernel,
        out_shape=shape((ep_size * duo, half, width + tag_width), BF16),
        in_specs=[vmem] * 3,
        out_specs=vmem,
        compiler_params=room(8192),
        name="spread",
    )(kept, met, tags)
    arrived = lax.all_to_all(
        outbound, BOTH, 0, 0, tiled=True, axis_index_groups=same_side
    )
    memory_next = (
        keep.reshape(seq_rows, 1, 1, 1) * memory
        + fresh[:, None, :, None] * values[:, None, None, :]
    )
    owned = pl.pallas_call(
        load_kernel,
        out_shape=tuple(shape(array.shape, array.dtype) for array in weights),
        in_specs=[hbm] * 3,
        out_specs=(vmem,) * 3,
        scratch_shapes=[pltpu.SemaphoreType.DMA((3,))],
        compiler_params=room(8192),
        name="loader",
    )(*[pltpu.with_memory_space_constraint(array, pltpu.HBM) for array in weights])
    blocks = pl.pallas_call(
        expert_kernel,
        out_shape=shape((ep_size * tp_size, half, quarter), BF16),
        in_specs=[vmem] * 8,
        out_specs=vmem,
        scratch_shapes=[
            pltpu.VMEM((ep_size * half, width), F32),
            pltpu.VMEM((ep_size * half, tag_width), F32),
        ],
        compiler_params=room(24576),
        name="experts",
    )(arrived, gain_moe.reshape(1, -1), *owned, *mates)
    returned = lax.all_to_all(blocks, BOTH, 0, 0, tiled=True)
    output = pl.pallas_call(
        combine_kernel,
        out_shape=shape((seq_rows, quarter), BF16),
        in_specs=[vmem],
        out_specs=vmem,
        compiler_params=room(16384),
        name="combine",
    )(returned)
    return (output, memory_next, norm_next, stab_row.T)


def solution(mesh):
    return jax.shard_map(
        shards,
        mesh=mesh,
        in_specs=(
            P("ep", None),
            P(None, "tp"),
            P(None, "tp"),
            P(None, "tp"),
            P(None, "tp"),
            P(None, "tp"),
            P(None, "tp"),
            P("tp"),
            P("tp", None),
            P(),
            P(),
            P("ep", "tp", None, None),
            P("ep", "tp", None),
            P("ep", "tp"),
            P("ep", None, "tp"),
            P("ep", None, "tp"),
            P("ep", "tp", None),
            P("ep", None),
            P("ep", None),
        ),
        out_specs=(P("ep", "tp"), P("ep", "tp", None, None), P("ep", "tp", None), P("ep", "tp")),
        check_vma=False,
    )
```

```python
import functools
import math

import jax
import jax.numpy as jnp
from jax import lax
from jax.experimental import pallas as pl
from jax.experimental.pallas import tpu as pltpu
from jax.sharding import PartitionSpec as P


BOTH = ("ep", "tp")
F32 = jnp.float32
BF16 = jnp.bfloat16


def dot(left, right):
    return jnp.dot(left, right, preferred_element_type=F32)


def normalize(values, gain_row):
    centered = values - jnp.mean(values, -1, keepdims=True)
    variance = jnp.mean(centered * centered, -1, keepdims=True)
    return centered * lax.rsqrt(variance + 1e-05) * gain_row


def eye_mask(size):
    rows = lax.broadcasted_iota(jnp.int32, (size, size), 0)
    return rows == lax.broadcasted_iota(jnp.int32, (size, size), 1)


def as_column(row):
    size = row.shape[1]
    spread = jnp.broadcast_to(row, (size, size))
    return jnp.sum(jnp.where(eye_mask(size), spread, 0.0), axis=1, keepdims=True)


def as_row(column):
    size = column.shape[0]
    spread = jnp.broadcast_to(column, (size, size))
    return jnp.sum(jnp.where(eye_mask(size), spread, 0.0), axis=0, keepdims=True)


def cell_kernel(
    bias,
    tokens_hbm,
    gain_hbm,
    w_in_hbm,
    w_forget_hbm,
    stabilizer_hbm,
    normalizer_hbm,
    wq_hbm,
    wk_hbm,
    wv_hbm,
    memory_hbm,
    wo_hbm,
    w_out_hbm,
    routes_hbm,
    route_weight_hbm,
    sent,
    kept,
    factors_out,
    row_factor,
    row_carry,
    norm_hbm,
    stabilizer_next_hbm,
    keep_out,
    fresh_out,
    values_out,
    tokens,
    gain,
    w_in,
    w_forget,
    stabilizer,
    normalizer,
    wq,
    wk,
    wv,
    memory,
    wo,
    w_out,
    routes,
    route_weight,
    norm_next,
    stabilizer_next,
    sems,
    write_sems,
):
    pairs = (
        (tokens_hbm, tokens),
        (gain_hbm, gain),
        (w_in_hbm, w_in),
        (w_forget_hbm, w_forget),
        (stabilizer_hbm, stabilizer),
        (normalizer_hbm, normalizer),
        (wq_hbm, wq),
        (wk_hbm, wk),
        (wv_hbm, wv),
        (wo_hbm, wo),
        (w_out_hbm, w_out),
        (routes_hbm, routes),
        (route_weight_hbm, route_weight),
        (memory_hbm, memory),
    )
    copies = [
        pltpu.make_async_copy(src, dst, sems.at[n]) for n, (src, dst) in enumerate(pairs)
    ]
    tp_id = lax.axis_index("tp")
    ep_id = lax.axis_index("ep")
    early = (0, 1, 2, 3, 4, 5, 11, 12)
    for n in early + (6, 7, 8, 13, 9, 10):
        copies[n].start()
    for n in early:
        copies[n].wait()
    seq_rows = tokens.shape[0]
    half = seq_rows // 2
    head_size = memory.shape[-1]
    token_rows = tokens[...].astype(F32)
    normed = normalize(token_rows, gain[...]).astype(BF16)
    wide = normed.astype(F32)
    gate_in = jnp.sum(wide * w_in[...].astype(F32), axis=1, keepdims=True)
    gate_forget = jnp.sum(wide * w_forget[...].astype(F32), axis=1, keepdims=True)
    logit = gate_forget + bias[0]
    log_forget = jnp.minimum(logit, 0.0) - jnp.log1p(jnp.exp(-jnp.abs(logit)))
    shifted = log_forget + as_column(stabilizer[...])
    stab = jnp.maximum(shifted, gate_in)
    keep = jnp.exp(shifted - stab)
    admit = jnp.exp(gate_in - stab)
    stabilizer_next[...] = as_row(stab)
    keep_out[...] = as_row(keep)
    writes = [
        pltpu.make_async_copy(stabilizer_next, stabilizer_next_hbm, write_sems.at[0]),
        pltpu.make_async_copy(norm_next, norm_hbm, write_sems.at[1]),
    ]
    writes[0].start()

    def project(number, weight):
        copies[number].wait()
        return dot(normed, weight[...]).astype(BF16).astype(F32)

    queries = project(6, wq)
    columns = queries.T
    keys = project(7, wk) * (1.0 / math.sqrt(head_size))
    values = project(8, wv)
    fresh = admit * keys
    grown = keep * normalizer[...].reshape(seq_rows, head_size) + fresh
    norm_next[...] = grown.reshape(norm_next.shape)
    writes[1].start()
    fresh_out[...] = fresh
    values_out[...] = values
    match = jnp.sum(queries * fresh, axis=1, keepdims=True)
    divisor = jnp.maximum(
        jnp.abs(jnp.sum(queries * grown, axis=1, keepdims=True)), jnp.exp(-stab)
    )
    named = routes[...].astype(F32)
    lanes = lax.broadcasted_iota(jnp.int32, factors_out.shape, 1)
    expert_of = lanes.astype(F32)
    share = jnp.zeros(lanes.shape, F32)
    for k in range(routes.shape[0]):
        share = share + jnp.where(
            expert_of == as_column(named[k : k + 1]), as_column(route_weight[k : k + 1]), 0.0
        )
    factors_out[...] = jnp.where(lanes == ep_id, 1.0, share)
    local = jnp.sum(jnp.where(lanes == ep_id, share, 0.0), axis=1, keepdims=True)
    local = jnp.where(tp_id & 1 == 0, local[:half], local[half:])
    row_count = row_factor.shape[0]
    local = jnp.concatenate([local] * (row_count // half), axis=0)
    owned = lax.broadcasted_iota(jnp.int32, row_factor.shape, 0) // half == ep_id
    row_factor[...] = jnp.where(owned, local, 1.0)
    row_carry[...] = jnp.where(owned & (tp_id < 2), 1.0, 0.0)
    copies[13].wait()
    recalled = []
    for s in range(seq_rows):
        recalled.append(jnp.sum(columns[:, s : s + 1] * memory[s, 0], axis=0, keepdims=True))
    old = jnp.concatenate(recalled, axis=0)
    readout = (keep * old + match * values) / divisor
    out_gate = project(9, wo)
    mixed = (jax.nn.sigmoid(out_gate) * readout).astype(BF16)
    copies[10].wait()
    head_part = dot(mixed, w_out[...])
    first = tp_id & 1 == 0
    own = head_part + jnp.where(tp_id < 2, 1.0, 0.0) * token_rows

    @pl.when(first)
    def _():
        sent[...] = head_part[half:].astype(BF16)
        kept[...] = own[:half]

    @pl.when(jnp.logical_not(first))
    def _():
        sent[...] = head_part[:half].astype(BF16)
        kept[...] = own[half:]

    for write in writes:
        write.wait()


def spread_kernel(kept, met, outbound):
    pair_sum = (kept[...] + met[...].astype(F32)).astype(BF16)
    for n in range(outbound.shape[0]):
        outbound[n] = pair_sum


def load_kernel(*refs):
    count = len(refs) // 2
    sems = refs[-1]
    copies = [
        pltpu.make_async_copy(refs[n], refs[count + n], sems.at[n]) for n in range(count)
    ]
    for copy in copies:
        copy.start()
    for copy in copies:
        copy.wait()


def expert_kernel(
    arrived,
    row_factor,
    row_carry,
    gain,
    gate_a,
    up_a,
    down_a,
    gate_b,
    up_b,
    down_b,
    blocks,
    residual,
):
    half, quarter = blocks.shape[1:]
    rows, width = residual.shape
    ep_size = rows // half
    duo = arrived.shape[0] // ep_size
    tp_size = width // quarter
    for e in range(ep_size):
        total = arrived[e * duo].astype(F32)
        for x in range(1, duo):
            total = total + arrived[e * duo + x].astype(F32)
        residual[e * half : (e + 1) * half, :] = total
    rows_in = normalize(residual[...], gain[...]).astype(BF16)

    def hidden(gate, up):
        both = dot(rows_in, jnp.concatenate([gate[...], up[...]], axis=1))
        gate_part, up_part = jnp.split(both, 2, axis=1)
        return (gate_part * jax.nn.sigmoid(gate_part) * up_part).astype(BF16)

    hiddens = jnp.concatenate([hidden(gate_a, up_a), hidden(gate_b, up_b)], axis=1)
    part = dot(hiddens, jnp.concatenate([down_a[...], down_b[...]], axis=0))
    part = row_factor[:, :1] * part + row_carry[:, :1] * residual[...]
    for e in range(ep_size):
        for t in range(tp_size):
            piece = part[e * half : (e + 1) * half, t * quarter : (t + 1) * quarter]
            blocks[e * tp_size + t] = piece.astype(BF16)


def combine_kernel(returned, factors, output, *, ep_size):
    half = returned.shape[1]
    tp_size = returned.shape[0] // ep_size
    for c in range(2):
        rows = slice(c * half, (c + 1) * half)
        total = 0.0
        for e in range(ep_size):
            value = returned[e * tp_size + c].astype(F32)
            for x in range(1, tp_size // 2):
                value = value + returned[e * tp_size + 2 * x + c].astype(F32)
            total = total + factors[rows, e : e + 1] * value
        output[rows, :] = total.astype(BF16)


def shards(
    tokens,
    w_query,
    w_key,
    w_value,
    w_outgate,
    w_igate,
    w_fgate,
    forget_bias,
    w_out,
    gain_mix,
    gain_moe,
    memory,
    normalizer,
    stabilizer,
    expert_gate,
    expert_up,
    expert_down,
    routes,
    route_weight,
):
    ep_size = lax.axis_size("ep")
    tp_size = lax.axis_size("tp")
    seq_rows, width = tokens.shape
    head_size = memory.shape[2]
    quarter = width // tp_size
    half = seq_rows // 2
    duo = tp_size // 2
    swap = [(t, t ^ 1) for t in range(tp_size)]
    same_side = [
        [e * tp_size + x * 2 + c for e in range(ep_size) for x in range(duo)] for c in range(2)
    ]
    smem = pl.BlockSpec(memory_space=pltpu.SMEM)
    vmem = pl.BlockSpec(memory_space=pltpu.VMEM)
    hbm = pl.BlockSpec(memory_space=pltpu.HBM)

    def room(kib):
        return pltpu.CompilerParams(vmem_limit_bytes=kib * 1024)

    shape = jax.ShapeDtypeStruct
    loads = (
        tokens,
        gain_mix.reshape(1, -1),
        w_igate.T,
        w_fgate.T,
        stabilizer.T,
        normalizer,
        w_query,
        w_key,
        w_value,
        memory,
        w_outgate,
        w_out,
        routes.T,
        route_weight.T,
    )
    lane_width = -(-ep_size // 128) * 128
    sent, kept, factors, row_factor, row_carry, norm_next, stab_row, keep, fresh, values = pl.pallas_call(
        cell_kernel,
        out_shape=(
            shape((half, width), BF16),
            shape((half, width), F32),
            shape((seq_rows, lane_width), F32),
            shape((ep_size * half, 128), F32),
            shape((ep_size * half, 128), F32),
            shape(normalizer.shape, F32),
            shape((1, seq_rows), F32),
            shape((1, seq_rows), F32),
            shape((seq_rows, head_size), F32),
            shape((seq_rows, head_size), F32),
        ),
        in_specs=[smem] + [hbm] * len(loads),
        out_specs=(vmem,) * 5 + (hbm,) * 2 + (vmem,) * 3,
        scratch_shapes=[pltpu.VMEM(array.shape, array.dtype) for array in loads]
        + [
            pltpu.VMEM(normalizer.shape, F32),
            pltpu.VMEM((1, seq_rows), F32),
            pltpu.SemaphoreType.DMA((len(loads),)),
            pltpu.SemaphoreType.DMA((2,)),
        ],
        compiler_params=room(20480),
        name="cell",
    )(
        forget_bias,
        *[pltpu.with_memory_space_constraint(array, pltpu.HBM) for array in loads],
    )
    weights = (expert_gate[0], expert_up[0], expert_down[0])
    sent, weights = lax.optimization_barrier((sent, weights))
    met = lax.ppermute(sent, "tp", swap)
    mates = [lax.ppermute(weight, "tp", swap) for weight in weights]
    outbound = pl.pallas_call(
        spread_kernel,
        out_shape=shape((ep_size * duo, half, width), BF16),
        in_specs=[vmem] * 2,
        out_specs=vmem,
        compiler_params=room(8192),
        name="spread",
    )(kept, met)
    arrived = lax.all_to_all(
        outbound, BOTH, 0, 0, tiled=True, axis_index_groups=same_side
    )
    memory_next = (
        keep.reshape(seq_rows, 1, 1, 1) * memory
        + fresh[:, None, :, None] * values[:, None, None, :]
    )
    owned = pl.pallas_call(
        load_kernel,
        out_shape=tuple(shape(array.shape, array.dtype) for array in weights),
        in_specs=[hbm] * 3,
        out_specs=(vmem,) * 3,
        scratch_shapes=[pltpu.SemaphoreType.DMA((3,))],
        compiler_params=room(8192),
        name="loader",
    )(*[pltpu.with_memory_space_constraint(array, pltpu.HBM) for array in weights])
    blocks = pl.pallas_call(
        expert_kernel,
        out_shape=shape((ep_size * tp_size, half, quarter), BF16),
        in_specs=[vmem] * 10,
        out_specs=vmem,
        scratch_shapes=[pltpu.VMEM((ep_size * half, width), F32)],
        compiler_params=room(24576),
        name="experts",
    )(arrived, row_factor, row_carry, gain_moe.reshape(1, -1), *owned, *mates)
    returned = lax.all_to_all(blocks, BOTH, 0, 0, tiled=True)
    output = pl.pallas_call(
        functools.partial(combine_kernel, ep_size=ep_size),
        out_shape=shape((seq_rows, quarter), BF16),
        in_specs=[vmem] * 2,
        out_specs=vmem,
        compiler_params=room(16384),
        name="combine",
    )(returned, factors)
    return (output, memory_next, norm_next, stab_row.T)


def solution(mesh):
    return jax.shard_map(
        shards,
        mesh=mesh,
        in_specs=(
            P("ep", None),
            P(None, "tp"),
            P(None, "tp"),
            P(None, "tp"),
            P(None, "tp"),
            P(None, "tp"),
            P(None, "tp"),
            P("tp"),
            P("tp", None),
            P(),
            P(),
            P("ep", "tp", None, None),
            P("ep", "tp", None),
            P("ep", "tp"),
            P("ep", None, "tp"),
            P("ep", None, "tp"),
            P("ep", "tp", None),
            P("ep", None),
            P("ep", None),
        ),
        out_specs=(P("ep", "tp"), P("ep", "tp", None, None), P("ep", "tp", None), P("ep", "tp")),
        check_vma=False,
    )
```

```python
import functools
import math

import jax
import jax.numpy as jnp
from jax import lax
from jax.experimental import pallas as pl
from jax.experimental.pallas import tpu as pltpu
from jax.sharding import PartitionSpec as P


BOTH = ("ep", "tp")
F32 = jnp.float32
BF16 = jnp.bfloat16


def dot(left, right):
    return jnp.dot(left, right, preferred_element_type=F32)


def normalize(values, gain_row):
    centered = values - jnp.mean(values, -1, keepdims=True)
    variance = jnp.mean(centered * centered, -1, keepdims=True)
    return centered * lax.rsqrt(variance + 1e-05) * gain_row


def eye_mask(size):
    rows = lax.broadcasted_iota(jnp.int32, (size, size), 0)
    return rows == lax.broadcasted_iota(jnp.int32, (size, size), 1)


def as_column(row):
    size = row.shape[1]
    spread = jnp.broadcast_to(row, (size, size))
    return jnp.sum(jnp.where(eye_mask(size), spread, 0.0), axis=1, keepdims=True)


def as_row(column):
    size = column.shape[0]
    spread = jnp.broadcast_to(column, (size, size))
    return jnp.sum(jnp.where(eye_mask(size), spread, 0.0), axis=0, keepdims=True)


def cell_kernel(
    bias,
    tokens_hbm,
    gain_hbm,
    w_in_hbm,
    w_forget_hbm,
    stabilizer_hbm,
    normalizer_hbm,
    wq_hbm,
    wk_hbm,
    wv_hbm,
    memory_hbm,
    wo_hbm,
    w_out_hbm,
    routes_hbm,
    route_weight_hbm,
    *rest,
    tp_size,
):
    sents, rest = rest[: tp_size - 1], rest[tp_size - 1 :]
    cell_body(
        bias,
        tokens_hbm,
        gain_hbm,
        w_in_hbm,
        w_forget_hbm,
        stabilizer_hbm,
        normalizer_hbm,
        wq_hbm,
        wk_hbm,
        wv_hbm,
        memory_hbm,
        wo_hbm,
        w_out_hbm,
        routes_hbm,
        route_weight_hbm,
        sents,
        *rest,
    )


def cell_body(
    bias,
    tokens_hbm,
    gain_hbm,
    w_in_hbm,
    w_forget_hbm,
    stabilizer_hbm,
    normalizer_hbm,
    wq_hbm,
    wk_hbm,
    wv_hbm,
    memory_hbm,
    wo_hbm,
    w_out_hbm,
    routes_hbm,
    route_weight_hbm,
    sents,
    kept,
    factors_out,
    row_factor,
    row_carry,
    norm_hbm,
    stabilizer_next_hbm,
    keep_out,
    fresh_out,
    values_out,
    tokens,
    gain,
    w_in,
    w_forget,
    stabilizer,
    normalizer,
    wq,
    wk,
    wv,
    memory,
    wo,
    w_out,
    routes,
    route_weight,
    norm_next,
    stabilizer_next,
    sems,
    write_sems,
):
    pairs = (
        (tokens_hbm, tokens),
        (gain_hbm, gain),
        (w_in_hbm, w_in),
        (w_forget_hbm, w_forget),
        (stabilizer_hbm, stabilizer),
        (normalizer_hbm, normalizer),
        (wq_hbm, wq),
        (wk_hbm, wk),
        (wv_hbm, wv),
        (wo_hbm, wo),
        (w_out_hbm, w_out),
        (routes_hbm, routes),
        (route_weight_hbm, route_weight),
        (memory_hbm, memory),
    )
    copies = [
        pltpu.make_async_copy(src, dst, sems.at[n]) for n, (src, dst) in enumerate(pairs)
    ]
    tp_id = lax.axis_index("tp")
    ep_id = lax.axis_index("ep")
    early = (0, 1, 2, 3, 4, 5, 11, 12)
    for n in early + (6, 7, 8, 13, 9, 10):
        copies[n].start()
    for n in early:
        copies[n].wait()
    seq_rows = tokens.shape[0]
    tp_size = len(sents) + 1
    portion = seq_rows // tp_size
    head_size = memory.shape[-1]
    token_rows = tokens[...].astype(F32)
    normed = normalize(token_rows, gain[...]).astype(BF16)
    wide = normed.astype(F32)
    gate_in = jnp.sum(wide * w_in[...].astype(F32), axis=1, keepdims=True)
    gate_forget = jnp.sum(wide * w_forget[...].astype(F32), axis=1, keepdims=True)
    logit = gate_forget + bias[0]
    log_forget = jnp.minimum(logit, 0.0) - jnp.log1p(jnp.exp(-jnp.abs(logit)))
    shifted = log_forget + as_column(stabilizer[...])
    stab = jnp.maximum(shifted, gate_in)
    keep = jnp.exp(shifted - stab)
    admit = jnp.exp(gate_in - stab)
    stabilizer_next[...] = as_row(stab)
    keep_out[...] = as_row(keep)
    writes = [
        pltpu.make_async_copy(stabilizer_next, stabilizer_next_hbm, write_sems.at[0]),
        pltpu.make_async_copy(norm_next, norm_hbm, write_sems.at[1]),
    ]
    writes[0].start()

    def project(number, weight):
        copies[number].wait()
        return dot(normed, weight[...]).astype(BF16).astype(F32)

    queries = project(6, wq)
    columns = queries.T
    keys = project(7, wk) * (1.0 / math.sqrt(head_size))
    values = project(8, wv)
    fresh = admit * keys
    grown = keep * normalizer[...].reshape(seq_rows, head_size) + fresh
    norm_next[...] = grown.reshape(norm_next.shape)
    writes[1].start()
    fresh_out[...] = fresh
    values_out[...] = values
    match = jnp.sum(queries * fresh, axis=1, keepdims=True)
    divisor = jnp.maximum(
        jnp.abs(jnp.sum(queries * grown, axis=1, keepdims=True)), jnp.exp(-stab)
    )
    named = routes[...].astype(F32)
    lanes = lax.broadcasted_iota(jnp.int32, factors_out.shape, 1)
    expert_of = lanes.astype(F32)
    share = jnp.zeros(lanes.shape, F32)
    for k in range(routes.shape[0]):
        share = share + jnp.where(
            expert_of == as_column(named[k : k + 1]), as_column(route_weight[k : k + 1]), 0.0
        )

    def side(array, c):
        return [array[portion * t : portion * (t + 1)] for t in range(c, tp_size, 2)]

    factors = jnp.where(lanes == ep_id, 1.0, share)
    factors_out[...] = jnp.concatenate(side(factors, 0) + side(factors, 1), axis=0)
    local = jnp.sum(jnp.where(lanes == ep_id, share, 0.0), axis=1, keepdims=True)
    local = jnp.where(
        tp_id & 1 == 0,
        jnp.concatenate(side(local, 0), axis=0),
        jnp.concatenate(side(local, 1), axis=0),
    )
    row_count = row_factor.shape[0]
    local = jnp.concatenate([local] * (row_count // local.shape[0]), axis=0)
    piece = lax.broadcasted_iota(jnp.int32, row_factor.shape, 0) // portion
    row_factor[...] = jnp.where(piece // (tp_size // 2) == ep_id, local, 1.0)
    row_carry[...] = jnp.where(piece == ep_id * (tp_size // 2) + (tp_id >> 1), 1.0, 0.0)
    copies[13].wait()
    recalled = []
    for s in range(seq_rows):
        recalled.append(jnp.sum(columns[:, s : s + 1] * memory[s, 0], axis=0, keepdims=True))
    old = jnp.concatenate(recalled, axis=0)
    readout = (keep * old + match * values) / divisor
    out_gate = project(9, wo)
    mixed = (jax.nn.sigmoid(out_gate) * readout).astype(BF16)
    copies[10].wait()
    head_part = dot(mixed, w_out[...])
    for t in range(tp_size):

        @pl.when(tp_id == t)
        def _():
            mine = slice(portion * t, portion * (t + 1))
            kept[...] = head_part[mine] + token_rows[mine]
            for r in range(1, tp_size):
                peer = t ^ r
                theirs = slice(portion * peer, portion * (peer + 1))
                sents[r - 1][...] = head_part[theirs].astype(BF16)

    for write in writes:
        write.wait()


def spread_kernel(kept, gain, *rest):
    mets, (residual_out, outbound) = rest[:-2], rest[-2:]
    residual = kept[...]
    for met in mets:
        residual = residual + met[...].astype(F32)
    residual_out[...] = residual
    normed = normalize(residual, gain[...]).astype(BF16)
    for n in range(outbound.shape[0]):
        outbound[n] = normed


def window_kernel(
    keep_row,
    fresh,
    values,
    memory_hbm,
    gate_hbm,
    up_hbm,
    down_hbm,
    memory_next,
    gate,
    up,
    down,
    memory,
    load_sems,
    read_sems,
    write_sems,
):
    count = memory.shape[0]
    reads = [
        pltpu.make_async_copy(memory_hbm.at[s], memory.at[s], read_sems.at[s])
        for s in range(count)
    ]
    for read in reads:
        read.start()
    pairs = ((gate_hbm, gate), (up_hbm, up), (down_hbm, down))
    loads = [
        pltpu.make_async_copy(src, dst, load_sems.at[n]) for n, (src, dst) in enumerate(pairs)
    ]
    for load in loads:
        load.start()
    keep = as_column(keep_row[...])
    columns = fresh[...].T
    writes = []
    for s in range(count):
        reads[s].wait()
        memory[s, 0] = (
            keep[s : s + 1] * memory[s, 0] + columns[:, s : s + 1] * values[s : s + 1, :]
        )
        write = pltpu.make_async_copy(memory.at[s], memory_next.at[s], write_sems.at[s])
        write.start()
        writes.append(write)
    for copy in loads + writes:
        copy.wait()


def expert_kernel(
    arrived,
    row_factor,
    row_carry,
    residual,
    gate_a,
    up_a,
    down_a,
    gate_b,
    up_b,
    down_b,
    blocks,
    gathered,
    repeated,
):
    half, quarter = blocks.shape[1:]
    rows, width = gathered.shape
    ep_size = rows // half
    portion = arrived.shape[1]
    tp_size = width // quarter
    for n in range(arrived.shape[0]):
        gathered[n * portion : (n + 1) * portion, :] = arrived[n].astype(F32)
    for n in range(repeated.shape[0] // portion):
        repeated[n * portion : (n + 1) * portion, :] = residual[...]
    rows_in = gathered[...].astype(BF16)

    def hidden(gate, up):
        both = dot(rows_in, jnp.concatenate([gate[...], up[...]], axis=1))
        gate_part, up_part = jnp.split(both, 2, axis=1)
        return (gate_part * jax.nn.sigmoid(gate_part) * up_part).astype(BF16)

    hiddens = jnp.concatenate([hidden(gate_a, up_a), hidden(gate_b, up_b)], axis=1)
    part = dot(hiddens, jnp.concatenate([down_a[...], down_b[...]], axis=0))
    carried = jnp.concatenate([repeated[...]] * (rows // repeated.shape[0]), axis=0)
    part = row_factor[:, :1] * part + row_carry[:, :1] * carried
    for e in range(ep_size):
        for t in range(tp_size):
            piece = part[e * half : (e + 1) * half, t * quarter : (t + 1) * quarter]
            blocks[e * tp_size + t] = piece.astype(BF16)


def combine_kernel(returned, factors, output, *, ep_size):
    half = returned.shape[1]
    tp_size = returned.shape[0] // ep_size
    portion = 2 * half // tp_size
    totals = []
    for c in range(2):
        rows = slice(c * half, (c + 1) * half)
        total = 0.0
        for e in range(ep_size):
            value = returned[e * tp_size + c].astype(F32)
            for x in range(1, tp_size // 2):
                value = value + returned[e * tp_size + 2 * x + c].astype(F32)
            total = total + factors[rows, e : e + 1] * value
        totals.append(total)
    pieces = [
        totals[t % 2][portion * (t // 2) : portion * (t // 2 + 1)] for t in range(tp_size)
    ]
    output[...] = jnp.concatenate(pieces, axis=0).astype(BF16)


def shards(
    tokens,
    w_query,
    w_key,
    w_value,
    w_outgate,
    w_igate,
    w_fgate,
    forget_bias,
    w_out,
    gain_mix,
    gain_moe,
    memory,
    normalizer,
    stabilizer,
    expert_gate,
    expert_up,
    expert_down,
    routes,
    route_weight,
):
    ep_size = lax.axis_size("ep")
    tp_size = lax.axis_size("tp")
    seq_rows, width = tokens.shape
    head_size = memory.shape[2]
    quarter = width // tp_size
    half = seq_rows // 2
    duo = tp_size // 2
    portion = seq_rows // tp_size
    swap = [(t, t ^ 1) for t in range(tp_size)]
    same_side = [
        [e * tp_size + x * 2 + c for e in range(ep_size) for x in range(duo)] for c in range(2)
    ]
    smem = pl.BlockSpec(memory_space=pltpu.SMEM)
    vmem = pl.BlockSpec(memory_space=pltpu.VMEM)
    hbm = pl.BlockSpec(memory_space=pltpu.HBM)

    def room(kib):
        return pltpu.CompilerParams(vmem_limit_bytes=kib * 1024)

    shape = jax.ShapeDtypeStruct
    loads = (
        tokens,
        gain_mix.reshape(1, -1),
        w_igate.T,
        w_fgate.T,
        stabilizer.T,
        normalizer,
        w_query,
        w_key,
        w_value,
        memory,
        w_outgate,
        w_out,
        routes.T,
        route_weight.T,
    )
    lane_width = -(-ep_size // 128) * 128
    peers = tp_size - 1
    results = pl.pallas_call(
        functools.partial(cell_kernel, tp_size=tp_size),
        out_shape=(
            *[shape((portion, width), BF16)] * peers,
            shape((portion, width), F32),
            shape((seq_rows, lane_width), F32),
            shape((ep_size * half, 128), F32),
            shape((ep_size * half, 128), F32),
            shape(normalizer.shape, F32),
            shape((1, seq_rows), F32),
            shape((1, seq_rows), F32),
            shape((seq_rows, head_size), F32),
            shape((seq_rows, head_size), F32),
        ),
        in_specs=[smem] + [hbm] * len(loads),
        out_specs=(vmem,) * (peers + 4) + (hbm,) * 2 + (vmem,) * 3,
        scratch_shapes=[pltpu.VMEM(array.shape, array.dtype) for array in loads]
        + [
            pltpu.VMEM(normalizer.shape, F32),
            pltpu.VMEM((1, seq_rows), F32),
            pltpu.SemaphoreType.DMA((len(loads),)),
            pltpu.SemaphoreType.DMA((2,)),
        ],
        compiler_params=room(20480),
        name="cell",
    )(
        forget_bias,
        *[pltpu.with_memory_space_constraint(array, pltpu.HBM) for array in loads],
    )
    sents, results = results[:peers], results[peers:]
    kept, factors, row_factor, row_carry, norm_next, stab_row, *state = results
    weights = (expert_gate[0], expert_up[0], expert_down[0])
    sents, weights = lax.optimization_barrier((sents, weights))
    mets = [
        lax.ppermute(sents[r - 1], "tp", [(t, t ^ r) for t in range(tp_size)])
        for r in range(1, tp_size)
    ]
    mates = [lax.ppermute(weight, "tp", swap) for weight in weights]
    residual, outbound = pl.pallas_call(
        spread_kernel,
        out_shape=(
            shape((portion, width), F32),
            shape((ep_size * duo, portion, width), BF16),
        ),
        in_specs=[vmem] * (peers + 2),
        out_specs=(vmem, vmem),
        compiler_params=room(8192),
        name="spread",
    )(kept, gain_moe.reshape(1, -1), *mets)
    arrived = lax.all_to_all(
        outbound, BOTH, 0, 0, tiled=True, axis_index_groups=same_side
    )
    memory_next, *owned = pl.pallas_call(
        window_kernel,
        out_shape=(
            shape(memory.shape, F32),
            *[shape(array.shape, array.dtype) for array in weights],
        ),
        in_specs=[vmem] * 3 + [hbm] * 4,
        out_specs=(hbm,) + (vmem,) * 3,
        scratch_shapes=[
            pltpu.VMEM(memory.shape, F32),
            pltpu.SemaphoreType.DMA((3,)),
            pltpu.SemaphoreType.DMA((seq_rows,)),
            pltpu.SemaphoreType.DMA((seq_rows,)),
        ],
        compiler_params=room(12288),
        name="keeper",
    )(
        *state,
        *[
            pltpu.with_memory_space_constraint(array, pltpu.HBM)
            for array in (memory, *weights)
        ],
    )
    blocks = pl.pallas_call(
        expert_kernel,
        out_shape=shape((ep_size * tp_size, half, quarter), BF16),
        in_specs=[vmem] * 10,
        out_specs=vmem,
        scratch_shapes=[
            pltpu.VMEM((ep_size * half, width), F32),
            pltpu.VMEM((8, width), F32),
        ],
        compiler_params=room(24576),
        name="experts",
    )(arrived, row_factor, row_carry, residual, *owned, *mates)
    returned = lax.all_to_all(blocks, BOTH, 0, 0, tiled=True)
    output = pl.pallas_call(
        functools.partial(combine_kernel, ep_size=ep_size),
        out_shape=shape((seq_rows, quarter), BF16),
        in_specs=[vmem] * 2,
        out_specs=vmem,
        compiler_params=room(16384),
        name="combine",
    )(returned, factors)
    return (output, memory_next, norm_next, stab_row.T)


def solution(mesh):
    return jax.shard_map(
        shards,
        mesh=mesh,
        in_specs=(
            P("ep", None),
            P(None, "tp"),
            P(None, "tp"),
            P(None, "tp"),
            P(None, "tp"),
            P(None, "tp"),
            P(None, "tp"),
            P("tp"),
            P("tp", None),
            P(),
            P(),
            P("ep", "tp", None, None),
            P("ep", "tp", None),
            P("ep", "tp"),
            P("ep", None, "tp"),
            P("ep", None, "tp"),
            P("ep", "tp", None),
            P("ep", None),
            P("ep", None),
        ),
        out_specs=(P("ep", "tp"), P("ep", "tp", None, None), P("ep", "tp", None), P("ep", "tp")),
        check_vma=False,
    )
```

```python
import functools
import math

import jax
import jax.numpy as jnp
from jax import lax
from jax.experimental import pallas as pl
from jax.experimental.pallas import tpu as pltpu
from jax.sharding import PartitionSpec as P


BOTH = ("ep", "tp")
F32 = jnp.float32
BF16 = jnp.bfloat16


def dot(left, right):
    return jnp.dot(left, right, preferred_element_type=F32)


def normalize(values, gain_row):
    centered = values - jnp.mean(values, -1, keepdims=True)
    variance = jnp.mean(centered * centered, -1, keepdims=True)
    return centered * lax.rsqrt(variance + 1e-05) * gain_row


def eye_mask(size):
    rows = lax.broadcasted_iota(jnp.int32, (size, size), 0)
    return rows == lax.broadcasted_iota(jnp.int32, (size, size), 1)


def as_column(row):
    size = row.shape[1]
    spread = jnp.broadcast_to(row, (size, size))
    return jnp.sum(jnp.where(eye_mask(size), spread, 0.0), axis=1, keepdims=True)


def as_row(column):
    size = column.shape[0]
    spread = jnp.broadcast_to(column, (size, size))
    return jnp.sum(jnp.where(eye_mask(size), spread, 0.0), axis=0, keepdims=True)


def cell_kernel(
    bias,
    tokens_hbm,
    gain_hbm,
    w_in_hbm,
    w_forget_hbm,
    stabilizer_hbm,
    normalizer_hbm,
    wq_hbm,
    wk_hbm,
    wv_hbm,
    memory_hbm,
    wo_hbm,
    w_out_hbm,
    routes_hbm,
    route_weight_hbm,
    *rest,
    tp_size,
):
    sents, rest = rest[: tp_size - 1], rest[tp_size - 1 :]
    cell_body(
        bias,
        tokens_hbm,
        gain_hbm,
        w_in_hbm,
        w_forget_hbm,
        stabilizer_hbm,
        normalizer_hbm,
        wq_hbm,
        wk_hbm,
        wv_hbm,
        memory_hbm,
        wo_hbm,
        w_out_hbm,
        routes_hbm,
        route_weight_hbm,
        sents,
        *rest,
    )


def cell_body(
    bias,
    tokens_hbm,
    gain_hbm,
    w_in_hbm,
    w_forget_hbm,
    stabilizer_hbm,
    normalizer_hbm,
    wq_hbm,
    wk_hbm,
    wv_hbm,
    memory_hbm,
    wo_hbm,
    w_out_hbm,
    routes_hbm,
    route_weight_hbm,
    sents,
    kept,
    factors_out,
    row_factor,
    row_carry,
    norm_hbm,
    stabilizer_next_hbm,
    memory_next,
    tokens,
    gain,
    w_in,
    w_forget,
    stabilizer,
    normalizer,
    wq,
    wk,
    wv,
    memory,
    wo,
    w_out,
    routes,
    route_weight,
    norm_next,
    stabilizer_next,
    sems,
    write_sems,
):
    pairs = (
        (tokens_hbm, tokens),
        (gain_hbm, gain),
        (w_in_hbm, w_in),
        (w_forget_hbm, w_forget),
        (stabilizer_hbm, stabilizer),
        (normalizer_hbm, normalizer),
        (wq_hbm, wq),
        (wk_hbm, wk),
        (wv_hbm, wv),
        (wo_hbm, wo),
        (w_out_hbm, w_out),
        (routes_hbm, routes),
        (route_weight_hbm, route_weight),
        (memory_hbm, memory),
    )
    copies = [
        pltpu.make_async_copy(src, dst, sems.at[n]) for n, (src, dst) in enumerate(pairs)
    ]
    tp_id = lax.axis_index("tp")
    ep_id = lax.axis_index("ep")
    early = (0, 1, 2, 3, 4, 5, 11, 12)
    for n in early + (6, 7, 8, 13, 9, 10):
        copies[n].start()
    for n in early:
        copies[n].wait()
    seq_rows = tokens.shape[0]
    tp_size = len(sents) + 1
    portion = seq_rows // tp_size
    head_size = memory.shape[-1]
    token_rows = tokens[...].astype(F32)
    normed = normalize(token_rows, gain[...]).astype(BF16)
    wide = normed.astype(F32)
    gate_in = jnp.sum(wide * w_in[...].astype(F32), axis=1, keepdims=True)
    gate_forget = jnp.sum(wide * w_forget[...].astype(F32), axis=1, keepdims=True)
    logit = gate_forget + bias[0]
    log_forget = jnp.minimum(logit, 0.0) - jnp.log1p(jnp.exp(-jnp.abs(logit)))
    shifted = log_forget + as_column(stabilizer[...])
    stab = jnp.maximum(shifted, gate_in)
    keep = jnp.exp(shifted - stab)
    admit = jnp.exp(gate_in - stab)
    stabilizer_next[...] = as_row(stab)
    writes = [
        pltpu.make_async_copy(stabilizer_next, stabilizer_next_hbm, write_sems.at[0]),
        pltpu.make_async_copy(norm_next, norm_hbm, write_sems.at[1]),
    ]
    writes[0].start()

    def project(number, weight):
        copies[number].wait()
        return dot(normed, weight[...]).astype(BF16).astype(F32)

    queries = project(6, wq)
    columns = queries.T
    keys = project(7, wk) * (1.0 / math.sqrt(head_size))
    values = project(8, wv)
    fresh = admit * keys
    grown = keep * normalizer[...].reshape(seq_rows, head_size) + fresh
    norm_next[...] = grown.reshape(norm_next.shape)
    writes[1].start()
    fresh_columns = fresh.T
    match = jnp.sum(queries * fresh, axis=1, keepdims=True)
    divisor = jnp.maximum(
        jnp.abs(jnp.sum(queries * grown, axis=1, keepdims=True)), jnp.exp(-stab)
    )
    named = routes[...].astype(F32)
    lanes = lax.broadcasted_iota(jnp.int32, factors_out.shape, 1)
    expert_of = lanes.astype(F32)
    share = jnp.zeros(lanes.shape, F32)
    for k in range(routes.shape[0]):
        share = share + jnp.where(
            expert_of == as_column(named[k : k + 1]), as_column(route_weight[k : k + 1]), 0.0
        )

    def side(array, c):
        return [array[portion * t : portion * (t + 1)] for t in range(c, tp_size, 2)]

    factors = jnp.where(lanes == ep_id, 1.0, share)
    factors_out[...] = jnp.concatenate(side(factors, 0) + side(factors, 1), axis=0)
    local = jnp.sum(jnp.where(lanes == ep_id, share, 0.0), axis=1, keepdims=True)
    local = jnp.where(
        tp_id & 1 == 0,
        jnp.concatenate(side(local, 0), axis=0),
        jnp.concatenate(side(local, 1), axis=0),
    )
    row_count = row_factor.shape[0]
    local = jnp.concatenate([local] * (row_count // local.shape[0]), axis=0)
    piece = lax.broadcasted_iota(jnp.int32, row_factor.shape, 0) // portion
    row_factor[...] = jnp.where(piece // (tp_size // 2) == ep_id, local, 1.0)
    row_carry[...] = jnp.where(piece == ep_id * (tp_size // 2) + (tp_id >> 1), 1.0, 0.0)
    copies[13].wait()
    recalled = []
    for s in range(seq_rows):
        matrix = memory[s, 0]
        recalled.append(jnp.sum(columns[:, s : s + 1] * matrix, axis=0, keepdims=True))
        memory[s, 0] = (
            keep[s : s + 1] * matrix + fresh_columns[:, s : s + 1] * values[s : s + 1]
        )
        write = pltpu.make_async_copy(memory.at[s], memory_next.at[s], write_sems.at[2 + s])
        write.start()
        writes.append(write)
    old = jnp.concatenate(recalled, axis=0)
    readout = (keep * old + match * values) / divisor
    out_gate = project(9, wo)
    mixed = (jax.nn.sigmoid(out_gate) * readout).astype(BF16)
    copies[10].wait()
    head_part = dot(mixed, w_out[...])
    for t in range(tp_size):

        @pl.when(tp_id == t)
        def _():
            mine = slice(portion * t, portion * (t + 1))
            kept[...] = head_part[mine] + token_rows[mine]
            for r in range(1, tp_size):
                peer = t ^ r
                theirs = slice(portion * peer, portion * (peer + 1))
                sents[r - 1][...] = head_part[theirs].astype(BF16)

    for write in writes:
        write.wait()


def spread_kernel(kept, gain, *rest):
    mets, (residual_out, outbound) = rest[:-2], rest[-2:]
    residual = kept[...]
    for met in mets:
        residual = residual + met[...].astype(F32)
    residual_out[...] = residual
    normed = normalize(residual, gain[...]).astype(BF16)
    for n in range(outbound.shape[0]):
        outbound[n] = normed


def expert_kernel(
    arrived,
    row_factor,
    row_carry,
    residual,
    gate_a,
    up_a,
    down_a,
    gate_b,
    up_b,
    down_b,
    blocks,
    gathered,
    repeated,
):
    half, quarter = blocks.shape[1:]
    rows, width = gathered.shape
    ep_size = rows // half
    portion = arrived.shape[1]
    tp_size = width // quarter
    for n in range(arrived.shape[0]):
        gathered[n * portion : (n + 1) * portion, :] = arrived[n].astype(F32)
    for n in range(repeated.shape[0] // portion):
        repeated[n * portion : (n + 1) * portion, :] = residual[...]
    rows_in = gathered[...].astype(BF16)

    def hidden(gate, up):
        both = dot(rows_in, jnp.concatenate([gate[...], up[...]], axis=1))
        gate_part, up_part = jnp.split(both, 2, axis=1)
        return (gate_part * jax.nn.sigmoid(gate_part) * up_part).astype(BF16)

    hiddens = jnp.concatenate([hidden(gate_a, up_a), hidden(gate_b, up_b)], axis=1)
    part = dot(hiddens, jnp.concatenate([down_a[...], down_b[...]], axis=0))
    carried = jnp.concatenate([repeated[...]] * (rows // repeated.shape[0]), axis=0)
    part = row_factor[:, :1] * part + row_carry[:, :1] * carried
    for e in range(ep_size):
        for t in range(tp_size):
            piece = part[e * half : (e + 1) * half, t * quarter : (t + 1) * quarter]
            blocks[e * tp_size + t] = piece.astype(BF16)


def combine_kernel(returned, factors, output, *, ep_size):
    half = returned.shape[1]
    tp_size = returned.shape[0] // ep_size
    portion = 2 * half // tp_size
    totals = []
    for c in range(2):
        rows = slice(c * half, (c + 1) * half)
        total = 0.0
        for e in range(ep_size):
            value = returned[e * tp_size + c].astype(F32)
            for x in range(1, tp_size // 2):
                value = value + returned[e * tp_size + 2 * x + c].astype(F32)
            total = total + factors[rows, e : e + 1] * value
        totals.append(total)
    pieces = [
        totals[t % 2][portion * (t // 2) : portion * (t // 2 + 1)] for t in range(tp_size)
    ]
    output[...] = jnp.concatenate(pieces, axis=0).astype(BF16)


def shards(
    tokens,
    w_query,
    w_key,
    w_value,
    w_outgate,
    w_igate,
    w_fgate,
    forget_bias,
    w_out,
    gain_mix,
    gain_moe,
    memory,
    normalizer,
    stabilizer,
    expert_gate,
    expert_up,
    expert_down,
    routes,
    route_weight,
):
    ep_size = lax.axis_size("ep")
    tp_size = lax.axis_size("tp")
    seq_rows, width = tokens.shape
    quarter = width // tp_size
    half = seq_rows // 2
    duo = tp_size // 2
    portion = seq_rows // tp_size
    swap = [(t, t ^ 1) for t in range(tp_size)]
    same_side = [
        [e * tp_size + x * 2 + c for e in range(ep_size) for x in range(duo)] for c in range(2)
    ]
    smem = pl.BlockSpec(memory_space=pltpu.SMEM)
    vmem = pl.BlockSpec(memory_space=pltpu.VMEM)
    hbm = pl.BlockSpec(memory_space=pltpu.HBM)

    def room(kib):
        return pltpu.CompilerParams(vmem_limit_bytes=kib * 1024)

    shape = jax.ShapeDtypeStruct
    loads = (
        tokens,
        gain_mix.reshape(1, -1),
        w_igate.T,
        w_fgate.T,
        stabilizer.T,
        normalizer,
        w_query,
        w_key,
        w_value,
        memory,
        w_outgate,
        w_out,
        routes.T,
        route_weight.T,
    )
    lane_width = -(-ep_size // 128) * 128
    peers = tp_size - 1
    results = pl.pallas_call(
        functools.partial(cell_kernel, tp_size=tp_size),
        out_shape=(
            *[shape((portion, width), BF16)] * peers,
            shape((portion, width), F32),
            shape((seq_rows, lane_width), F32),
            shape((ep_size * half, 128), F32),
            shape((ep_size * half, 128), F32),
            shape(normalizer.shape, F32),
            shape((1, seq_rows), F32),
            shape(memory.shape, F32),
        ),
        in_specs=[smem] + [hbm] * len(loads),
        out_specs=(vmem,) * (peers + 4) + (hbm,) * 3,
        scratch_shapes=[pltpu.VMEM(array.shape, array.dtype) for array in loads]
        + [
            pltpu.VMEM(normalizer.shape, F32),
            pltpu.VMEM((1, seq_rows), F32),
            pltpu.SemaphoreType.DMA((len(loads),)),
            pltpu.SemaphoreType.DMA((2 + seq_rows,)),
        ],
        compiler_params=room(20480),
        name="cell",
    )(
        forget_bias,
        *[pltpu.with_memory_space_constraint(array, pltpu.HBM) for array in loads],
    )
    sents, results = results[:peers], results[peers:]
    kept, factors, row_factor, row_carry, norm_next, stab_row, memory_next = results
    weights = (expert_gate[0], expert_up[0], expert_down[0])
    sents, weights = lax.optimization_barrier((sents, weights))
    mets = [
        lax.ppermute(sents[r - 1], "tp", [(t, t ^ r) for t in range(tp_size)])
        for r in range(tp_size - 1, 0, -1)
    ]
    mates = [lax.ppermute(weight, "tp", swap) for weight in weights]
    residual, outbound = pl.pallas_call(
        spread_kernel,
        out_shape=(
            shape((portion, width), F32),
            shape((ep_size * duo, portion, width), BF16),
        ),
        in_specs=[vmem] * (peers + 2),
        out_specs=(vmem, vmem),
        compiler_params=room(8192),
        name="spread",
    )(kept, gain_moe.reshape(1, -1), *mets)
    arrived = lax.all_to_all(
        outbound, BOTH, 0, 0, tiled=True, axis_index_groups=same_side
    )
    blocks = pl.pallas_call(
        expert_kernel,
        out_shape=shape((ep_size * tp_size, half, quarter), BF16),
        in_specs=[vmem] * 10,
        out_specs=vmem,
        scratch_shapes=[
            pltpu.VMEM((ep_size * half, width), F32),
            pltpu.VMEM((8, width), F32),
        ],
        compiler_params=room(24576),
        name="experts",
    )(arrived, row_factor, row_carry, residual, *weights, *mates)
    returned = lax.all_to_all(blocks, BOTH, 0, 0, tiled=True)
    output = pl.pallas_call(
        functools.partial(combine_kernel, ep_size=ep_size),
        out_shape=shape((seq_rows, quarter), BF16),
        in_specs=[vmem] * 2,
        out_specs=vmem,
        compiler_params=room(16384),
        name="combine",
    )(returned, factors)
    return (output, memory_next, norm_next, stab_row.T)


def solution(mesh):
    return jax.shard_map(
        shards,
        mesh=mesh,
        in_specs=(
            P("ep", None),
            P(None, "tp"),
            P(None, "tp"),
            P(None, "tp"),
            P(None, "tp"),
            P(None, "tp"),
            P(None, "tp"),
            P("tp"),
            P("tp", None),
            P(),
            P(),
            P("ep", "tp", None, None),
            P("ep", "tp", None),
            P("ep", "tp"),
            P("ep", None, "tp"),
            P("ep", None, "tp"),
            P("ep", "tp", None),
            P("ep", None),
            P("ep", None),
        ),
        out_specs=(P("ep", "tp"), P("ep", "tp", None, None), P("ep", "tp", None), P("ep", "tp")),
        check_vma=False,
    )
```

```python
import functools
import math

import jax
import jax.numpy as jnp
from jax import lax
from jax.experimental import pallas as pl
from jax.experimental.pallas import tpu as pltpu
from jax.sharding import PartitionSpec as P


BOTH = ("ep", "tp")
F32 = jnp.float32
BF16 = jnp.bfloat16


def dot(left, right):
    return jnp.dot(left, right, preferred_element_type=F32)


def normalize(values, gain_row):
    centered = values - jnp.mean(values, -1, keepdims=True)
    variance = jnp.mean(centered * centered, -1, keepdims=True)
    return centered * lax.rsqrt(variance + 1e-05) * gain_row


def eye_mask(size):
    rows = lax.broadcasted_iota(jnp.int32, (size, size), 0)
    return rows == lax.broadcasted_iota(jnp.int32, (size, size), 1)


def as_column(row):
    size = row.shape[1]
    spread = jnp.broadcast_to(row, (size, size))
    return jnp.sum(jnp.where(eye_mask(size), spread, 0.0), axis=1, keepdims=True)


def as_row(column):
    size = column.shape[0]
    spread = jnp.broadcast_to(column, (size, size))
    return jnp.sum(jnp.where(eye_mask(size), spread, 0.0), axis=0, keepdims=True)


def cell_kernel(
    bias,
    tokens_hbm,
    gain_hbm,
    w_in_hbm,
    w_forget_hbm,
    stabilizer_hbm,
    normalizer_hbm,
    wq_hbm,
    wk_hbm,
    wv_hbm,
    memory_hbm,
    wo_hbm,
    w_out_hbm,
    routes_hbm,
    route_weight_hbm,
    *rest,
    tp_size,
):
    sents, rest = rest[: tp_size - 1], rest[tp_size - 1 :]
    cell_body(
        bias,
        tokens_hbm,
        gain_hbm,
        w_in_hbm,
        w_forget_hbm,
        stabilizer_hbm,
        normalizer_hbm,
        wq_hbm,
        wk_hbm,
        wv_hbm,
        memory_hbm,
        wo_hbm,
        w_out_hbm,
        routes_hbm,
        route_weight_hbm,
        sents,
        *rest,
    )


def cell_body(
    bias,
    tokens_hbm,
    gain_hbm,
    w_in_hbm,
    w_forget_hbm,
    stabilizer_hbm,
    normalizer_hbm,
    wq_hbm,
    wk_hbm,
    wv_hbm,
    memory_hbm,
    wo_hbm,
    w_out_hbm,
    routes_hbm,
    route_weight_hbm,
    sents,
    kept,
    factors_out,
    row_factor,
    row_carry,
    norm_hbm,
    stabilizer_next_hbm,
    memory_next,
    tokens,
    gain,
    w_in,
    w_forget,
    stabilizer,
    normalizer,
    wq,
    wk,
    wv,
    memory,
    wo,
    w_out,
    routes,
    route_weight,
    norm_next,
    stabilizer_next,
    sems,
    write_sems,
):
    pairs = (
        (tokens_hbm, tokens),
        (gain_hbm, gain),
        (w_in_hbm, w_in),
        (w_forget_hbm, w_forget),
        (stabilizer_hbm, stabilizer),
        (normalizer_hbm, normalizer),
        (wq_hbm, wq),
        (wk_hbm, wk),
        (wv_hbm, wv),
        (wo_hbm, wo),
        (w_out_hbm, w_out),
        (routes_hbm, routes),
        (route_weight_hbm, route_weight),
        (memory_hbm, memory),
    )
    copies = [
        pltpu.make_async_copy(src, dst, sems.at[n]) for n, (src, dst) in enumerate(pairs)
    ]
    tp_id = lax.axis_index("tp")
    ep_id = lax.axis_index("ep")
    early = (0, 1, 2, 3, 4, 5, 11, 12)
    for n in early + (6, 7, 8, 13, 9, 10):
        copies[n].start()
    for n in early:
        copies[n].wait()
    seq_rows = tokens.shape[0]
    tp_size = len(sents) + 1
    portion = seq_rows // tp_size
    head_size = memory.shape[-1]
    token_rows = tokens[...].astype(F32)
    normed = normalize(token_rows, gain[...]).astype(BF16)
    wide = normed.astype(F32)
    gate_in = jnp.sum(wide * w_in[...].astype(F32), axis=1, keepdims=True)
    gate_forget = jnp.sum(wide * w_forget[...].astype(F32), axis=1, keepdims=True)
    logit = gate_forget + bias[0]
    log_forget = jnp.minimum(logit, 0.0) - jnp.log1p(jnp.exp(-jnp.abs(logit)))
    shifted = log_forget + as_column(stabilizer[...])
    stab = jnp.maximum(shifted, gate_in)
    keep = jnp.exp(shifted - stab)
    admit = jnp.exp(gate_in - stab)
    stabilizer_next[...] = as_row(stab)
    writes = [
        pltpu.make_async_copy(stabilizer_next, stabilizer_next_hbm, write_sems.at[0]),
        pltpu.make_async_copy(norm_next, norm_hbm, write_sems.at[1]),
    ]
    writes[0].start()

    def project(number, weight):
        copies[number].wait()
        return dot(normed, weight[...]).astype(BF16).astype(F32)

    queries = project(6, wq)
    columns = queries.T
    keys = project(7, wk) * (1.0 / math.sqrt(head_size))
    values = project(8, wv)
    fresh = admit * keys
    grown = keep * normalizer[...].reshape(seq_rows, head_size) + fresh
    norm_next[...] = grown.reshape(norm_next.shape)
    writes[1].start()
    fresh_columns = fresh.T
    match = jnp.sum(queries * fresh, axis=1, keepdims=True)
    divisor = jnp.maximum(
        jnp.abs(jnp.sum(queries * grown, axis=1, keepdims=True)), jnp.exp(-stab)
    )
    named = routes[...].astype(F32)
    lane_width = -(-factors_out.shape[0] // 128) * 128
    lanes = lax.broadcasted_iota(jnp.int32, (seq_rows, lane_width), 1)
    expert_of = lanes.astype(F32)
    share = jnp.zeros(lanes.shape, F32)
    for k in range(routes.shape[0]):
        share = share + jnp.where(
            expert_of == as_column(named[k : k + 1]), as_column(route_weight[k : k + 1]), 0.0
        )

    def side(array, c):
        return [array[portion * t : portion * (t + 1)] for t in range(c, tp_size, 2)]

    factors = jnp.where(lanes == ep_id, 1.0, share)
    ordered = jnp.concatenate(side(factors, 0) + side(factors, 1), axis=0)
    for e in range(factors_out.shape[0]):
        factors_out[e] = jnp.broadcast_to(ordered[:, e : e + 1], factors_out.shape[1:])
    local = jnp.sum(jnp.where(lanes == ep_id, share, 0.0), axis=1, keepdims=True)
    local = jnp.where(
        tp_id & 1 == 0,
        jnp.concatenate(side(local, 0), axis=0),
        jnp.concatenate(side(local, 1), axis=0),
    )
    row_count = row_factor.shape[0]
    local = jnp.concatenate([local] * (row_count // local.shape[0]), axis=0)
    piece = lax.broadcasted_iota(jnp.int32, row_factor.shape, 0) // portion
    row_factor[...] = jnp.where(piece // (tp_size // 2) == ep_id, local, 1.0)
    row_carry[...] = jnp.where(piece == ep_id * (tp_size // 2) + (tp_id >> 1), 1.0, 0.0)
    copies[13].wait()
    recalled = []
    for s in range(seq_rows):
        matrix = memory[s, 0]
        recalled.append(jnp.sum(columns[:, s : s + 1] * matrix, axis=0, keepdims=True))
        memory[s, 0] = (
            keep[s : s + 1] * matrix + fresh_columns[:, s : s + 1] * values[s : s + 1]
        )
        write = pltpu.make_async_copy(memory.at[s], memory_next.at[s], write_sems.at[2 + s])
        write.start()
        writes.append(write)
    old = jnp.concatenate(recalled, axis=0)
    readout = (keep * old + match * values) / divisor
    out_gate = project(9, wo)
    mixed = (jax.nn.sigmoid(out_gate) * readout).astype(BF16)
    copies[10].wait()
    head_part = dot(mixed, w_out[...])
    for t in range(tp_size):

        @pl.when(tp_id == t)
        def _():
            mine = slice(portion * t, portion * (t + 1))
            kept[...] = head_part[mine] + token_rows[mine]
            for r in range(1, tp_size):
                peer = t ^ r
                theirs = slice(portion * peer, portion * (peer + 1))
                sents[r - 1][...] = head_part[theirs].astype(BF16)

    for write in writes:
        write.wait()


def spread_kernel(kept, gain, *rest):
    mets, (residual_out, outbound) = rest[:-2], rest[-2:]
    residual = kept[...]
    for met in mets:
        residual = residual + met[...].astype(F32)
    residual_out[...] = residual
    normed = normalize(residual, gain[...]).astype(BF16)
    for n in range(outbound.shape[0]):
        outbound[n] = normed


def expert_kernel(
    arrived,
    row_factor,
    row_carry,
    residual,
    gate_a,
    up_a,
    down_a,
    gate_b,
    up_b,
    down_b,
    blocks,
    gathered,
    repeated,
):
    half, quarter = blocks.shape[1:]
    rows, width = gathered.shape
    ep_size = rows // half
    portion = arrived.shape[1]
    tp_size = width // quarter
    for n in range(arrived.shape[0]):
        gathered[n * portion : (n + 1) * portion, :] = arrived[n].astype(F32)
    for n in range(repeated.shape[0] // portion):
        repeated[n * portion : (n + 1) * portion, :] = residual[...]
    rows_in = gathered[...].astype(BF16)

    def hidden(gate, up):
        both = dot(rows_in, jnp.concatenate([gate[...], up[...]], axis=1))
        gate_part, up_part = jnp.split(both, 2, axis=1)
        return (gate_part * jax.nn.sigmoid(gate_part) * up_part).astype(BF16)

    hiddens = jnp.concatenate([hidden(gate_a, up_a), hidden(gate_b, up_b)], axis=1)
    part = dot(hiddens, jnp.concatenate([down_a[...], down_b[...]], axis=0))
    carried = jnp.concatenate([repeated[...]] * (rows // repeated.shape[0]), axis=0)
    part = row_factor[:, :1] * part + row_carry[:, :1] * carried
    for e in range(ep_size):
        for t in range(tp_size):
            piece = part[e * half : (e + 1) * half, t * quarter : (t + 1) * quarter]
            blocks[e * tp_size + t] = piece.astype(BF16)


def combine_kernel(returned, factors, output, *, ep_size):
    half = returned.shape[1]
    tp_size = returned.shape[0] // ep_size
    portion = 2 * half // tp_size
    totals = []
    for c in range(2):
        rows = slice(c * half, (c + 1) * half)
        total = 0.0
        for e in range(ep_size):
            value = returned[e * tp_size + c].astype(F32)
            for x in range(1, tp_size // 2):
                value = value + returned[e * tp_size + 2 * x + c].astype(F32)
            factor = jnp.concatenate([factors[e, rows, :]] * (value.shape[1] // 128), axis=1)
            total = total + factor * value
        totals.append(total)
    pieces = [
        totals[t % 2][portion * (t // 2) : portion * (t // 2 + 1)] for t in range(tp_size)
    ]
    output[...] = jnp.concatenate(pieces, axis=0).astype(BF16)


def shards(
    tokens,
    w_query,
    w_key,
    w_value,
    w_outgate,
    w_igate,
    w_fgate,
    forget_bias,
    w_out,
    gain_mix,
    gain_moe,
    memory,
    normalizer,
    stabilizer,
    expert_gate,
    expert_up,
    expert_down,
    routes,
    route_weight,
):
    ep_size = lax.axis_size("ep")
    tp_size = lax.axis_size("tp")
    seq_rows, width = tokens.shape
    quarter = width // tp_size
    half = seq_rows // 2
    duo = tp_size // 2
    portion = seq_rows // tp_size
    swap = [(t, t ^ 1) for t in range(tp_size)]
    same_side = [
        [e * tp_size + x * 2 + c for e in range(ep_size) for x in range(duo)] for c in range(2)
    ]
    smem = pl.BlockSpec(memory_space=pltpu.SMEM)
    vmem = pl.BlockSpec(memory_space=pltpu.VMEM)
    hbm = pl.BlockSpec(memory_space=pltpu.HBM)

    def room(kib):
        return pltpu.CompilerParams(vmem_limit_bytes=kib * 1024)

    shape = jax.ShapeDtypeStruct
    loads = (
        tokens,
        gain_mix.reshape(1, -1),
        w_igate.T,
        w_fgate.T,
        stabilizer.T,
        normalizer,
        w_query,
        w_key,
        w_value,
        memory,
        w_outgate,
        w_out,
        routes.T,
        route_weight.T,
    )
    peers = tp_size - 1
    results = pl.pallas_call(
        functools.partial(cell_kernel, tp_size=tp_size),
        out_shape=(
            *[shape((portion, width), BF16)] * peers,
            shape((portion, width), F32),
            shape((ep_size, seq_rows, 128), F32),
            shape((ep_size * half, 128), F32),
            shape((ep_size * half, 128), F32),
            shape(normalizer.shape, F32),
            shape((1, seq_rows), F32),
            shape(memory.shape, F32),
        ),
        in_specs=[smem] + [hbm] * len(loads),
        out_specs=(vmem,) * (peers + 4) + (hbm,) * 3,
        scratch_shapes=[pltpu.VMEM(array.shape, array.dtype) for array in loads]
        + [
            pltpu.VMEM(normalizer.shape, F32),
            pltpu.VMEM((1, seq_rows), F32),
            pltpu.SemaphoreType.DMA((len(loads),)),
            pltpu.SemaphoreType.DMA((2 + seq_rows,)),
        ],
        compiler_params=room(20480),
        name="cell",
    )(
        forget_bias,
        *[pltpu.with_memory_space_constraint(array, pltpu.HBM) for array in loads],
    )
    sents, results = results[:peers], results[peers:]
    kept, factors, row_factor, row_carry, norm_next, stab_row, memory_next = results
    weights = (expert_gate[0], expert_up[0], expert_down[0])
    sents, weights = lax.optimization_barrier((sents, weights))
    mets = [
        lax.ppermute(sents[r - 1], "tp", [(t, t ^ r) for t in range(tp_size)])
        for r in range(tp_size - 1, 0, -1)
    ]
    mates = [lax.ppermute(weight, "tp", swap) for weight in weights]
    residual, outbound = pl.pallas_call(
        spread_kernel,
        out_shape=(
            shape((portion, width), F32),
            shape((ep_size * duo, portion, width), BF16),
        ),
        in_specs=[vmem] * (peers + 2),
        out_specs=(vmem, vmem),
        compiler_params=room(8192),
        name="spread",
    )(kept, gain_moe.reshape(1, -1), *mets)
    arrived = lax.all_to_all(
        outbound, BOTH, 0, 0, tiled=True, axis_index_groups=same_side
    )
    blocks = pl.pallas_call(
        expert_kernel,
        out_shape=shape((ep_size * tp_size, half, quarter), BF16),
        in_specs=[vmem] * 10,
        out_specs=vmem,
        scratch_shapes=[
            pltpu.VMEM((ep_size * half, width), F32),
            pltpu.VMEM((8, width), F32),
        ],
        compiler_params=room(24576),
        name="experts",
    )(arrived, row_factor, row_carry, residual, *weights, *mates)
    returned = lax.all_to_all(blocks, BOTH, 0, 0, tiled=True)
    output = pl.pallas_call(
        functools.partial(combine_kernel, ep_size=ep_size),
        out_shape=shape((seq_rows, quarter), BF16),
        in_specs=[vmem] * 2,
        out_specs=vmem,
        compiler_params=room(16384),
        name="combine",
    )(returned, factors)
    return (output, memory_next, norm_next, stab_row.T)


def solution(mesh):
    return jax.shard_map(
        shards,
        mesh=mesh,
        in_specs=(
            P("ep", None),
            P(None, "tp"),
            P(None, "tp"),
            P(None, "tp"),
            P(None, "tp"),
            P(None, "tp"),
            P(None, "tp"),
            P("tp"),
            P("tp", None),
            P(),
            P(),
            P("ep", "tp", None, None),
            P("ep", "tp", None),
            P("ep", "tp"),
            P("ep", None, "tp"),
            P("ep", None, "tp"),
            P("ep", "tp", None),
            P("ep", None),
            P("ep", None),
        ),
        out_specs=(P("ep", "tp"), P("ep", "tp", None, None), P("ep", "tp", None), P("ep", "tp")),
        check_vma=False,
    )
```
